32 devices in a mesh: grp: 2 (over y), kv: 4 (over z), tp: 4 (over x, core).
Axes of the slice: x: 2, y: 2, z: 4, core: 2. Of those that a mesh axis runs over, the one named last changes fastest.
Arguments:
- tokens: bfloat16 [32, 4096], P('grp', 'kv'), parts along dimension 0, may hold values from -16 to 16
- positions: int32 [32], P(('grp', 'kv')), parts along dimension 0, may hold values from 512 to 8191
- state: float32 [32, 16, 128, 128], P(('grp', 'kv'), 'tp'), parts along dimension 0, may hold values from -3 to 3
- norm_gain: float32 [4096], P('kv'), may hold values from 0.1 to 1.9
- w_query: bfloat16 [4096, 2048], P('kv', 'tp'), may hold values from -0.09375 to 0.09375
- w_key: bfloat16 [4096, 2048], P('kv', 'tp'), may hold values from -0.09375 to 0.09375
- w_value: bfloat16 [4096, 2048], P('kv', 'tp'), may hold values from -0.09375 to 0.09375
- w_gate: bfloat16 [4096, 2048], P('kv', 'tp'), may hold values from -0.09375 to 0.09375
- w_out: bfloat16 [2048, 4096], P('tp', 'kv'), may hold values from -0.125 to 0.125
- mlp_gain: float32 [4096], P('kv'), may hold values from 0.1 to 1.9
- w_up: bfloat16 [4096, 16384], P('kv', 'tp'), may hold values from -0.09375 to 0.09375
- w_down: bfloat16 [16384, 4096], P('tp', 'kv'), may hold values from -0.046875 to 0.046875
Outputs:
- layer_out: bfloat16 [32, 4096], P('grp', 'kv'), parts along dimension 0
- new_state: float32 [32, 16, 128, 128], P(('grp', 'kv'), 'tp'), parts along dimension 0
The draws below stay inside these ranges and needn't reach their ends.
There are 2 independent parts, one for each index of `grp`. The reference program is written for one: setup_inputs(seed, part) draws one part's arguments, and reference() takes and returns one part's arrays. A program takes and returns all parts, laid end to end along the dimension named above; an argument that names none is the same for every part. Nothing has to cross between parts.
All inputs are finite; a program needn't handle non-finite values.
Results may differ from the reference program's by a relative error of at most 0.007.
Values may be sent and summed in bfloat16 or wider, within the bound.
No kernel may reach another device: no remote copies, remote signals or barrier semaphores. Data moves between devices by JAX's collectives and lax.ppermute only.
A program may use at most 64 MiB of HBM per device.

```python
import jax
import jax.numpy as jnp
from jax import lax

D = 4096
HEADS = 16
HEAD_DIM = 128
FF = 16384
BATCH = 16
RET = 2048


def draw_tokens(key, part):
    first = jax.random.fold_in(jax.random.fold_in(key, 11), 0)
    columns = jnp.exp(jnp.log(4.0) * jnp.arange(D, dtype=jnp.float32) / D) * 0.5
    base = jnp.clip(jax.random.normal(first, (BATCH, D), jnp.float32), -4.0, 4.0)
    values = base * columns[None, :]
    return values.astype(jnp.bfloat16)


def with_ends(values, own_key, low, top_value):
    longest = values.shape.index(max(values.shape))
    spots = []
    for shift in (0, 1):
        where = [jax.random.randint(jax.random.fold_in(own_key, axis), (), 0, length) for axis, length in enumerate(values.shape)]
        where[longest] = (where[longest] + shift) % values.shape[longest]
        spots.append(tuple(where))
    return values.at[spots[0]].set(low).at[spots[1]].set(top_value)


def block_scale(rng, shape, pieces, least, largest):
    def one(axis_at, blocks):
        steps = jax.random.uniform(jax.random.fold_in(jax.random.fold_in(rng, 6), axis_at), (blocks,), jnp.float32, least / len(pieces), largest / len(pieces))
        return jnp.repeat(jnp.exp(steps), shape[axis_at] // blocks).reshape((-1,) + (1,) * (len(shape) - axis_at - 1))

    level = one(*pieces[0])
    for cut in pieces[1:]:
        level = level * one(*cut)
    return level


def centred(key, dims, deviation, most, pieces=(), kind=jnp.bfloat16):
    values = deviation * jax.random.normal(key, dims, jnp.float32)
    if pieces:
        values = values * block_scale(key, dims, pieces, -0.22, 0.18)
    return jnp.clip(values, -most, most).astype(kind)


def setup_inputs(seed: int = 0, part: int = 0) -> dict:
    splits = jax.random.split(jax.random.key(seed), 13)
    part_keys = jax.random.split(jax.random.fold_in(splits[12], part), 13)
    tokens = draw_tokens(jax.random.fold_in(jax.random.fold_in(splits[12], part), 71), part)
    positions = with_ends(jax.random.randint(part_keys[1], (BATCH,), 512, 8192), jax.random.fold_in(part_keys[1], 1), 512, 8191).astype(jnp.int32)
    state = centred(part_keys[2], (BATCH, HEADS, HEAD_DIM, HEAD_DIM), 0.5, 3.0, ((0, 4), (1, 4)), jnp.float32)
    norm_gain = jnp.clip(1.0 + 0.18 * jax.random.normal(splits[3], (D,), jnp.float32), 0.1, 1.9)
    w_query = centred(splits[4], (D, RET), D ** -0.5, 0.09375, ((0, 4), (1, 4)))
    w_key = centred(splits[5], (D, RET), D ** -0.5, 0.09375, ((0, 4), (1, 4)))
    w_value = centred(splits[6], (D, RET), D ** -0.5, 0.09375, ((0, 4), (1, 4)))
    w_gate = centred(splits[7], (D, RET), D ** -0.5, 0.09375, ((0, 4), (1, 4)))
    w_out = centred(splits[8], (RET, D), RET ** -0.5, 0.125, ((0, 4), (1, 4)))
    mlp_gain = jnp.clip(1.0 + 0.18 * jax.random.normal(splits[9], (D,), jnp.float32), 0.1, 1.9)
    w_up = centred(splits[10], (D, FF), D ** -0.5, 0.09375, ((0, 4), (1, 4)))
    w_down = centred(splits[11], (FF, D), FF ** -0.5, 0.046875, ((0, 4), (1, 4)))
    return dict(tokens=tokens, positions=positions, state=state, norm_gain=norm_gain, w_query=w_query, w_key=w_key, w_value=w_value, w_gate=w_gate, w_out=w_out, mlp_gain=mlp_gain, w_up=w_up, w_down=w_down)


def turn(values, positions):
    half = values.shape[-1] // 2
    freq = 10000.0 ** (-(jnp.arange(half, dtype=jnp.float32) * 2.0) / values.shape[-1])
    angle = positions.astype(jnp.float32)[:, None, None] * freq[None, None, :]
    cosine = jnp.cos(angle)
    sine = jnp.sin(angle)
    first = values[..., :half]
    second = values[..., half:]
    return jnp.concatenate([first * cosine - second * sine, first * sine + second * cosine], axis=-1)

def reference(tokens, positions, state, norm_gain, w_query, w_key, w_value, w_gate, w_out, mlp_gain, w_up, w_down):
    rows = tokens.shape[0]
    inputs = tokens.astype(jnp.float32)
    scale1 = lax.rsqrt(lax.optimization_barrier(jnp.mean(inputs * inputs, axis=1)) + 1e-06)
    normed = (inputs * norm_gain).astype(jnp.bfloat16)

    def project(weight):
        raw = jnp.dot(normed, weight, preferred_element_type=jnp.float32) * scale1[:, None]
        return raw.reshape(rows, HEADS, HEAD_DIM)
    query = turn(project(w_query), positions)
    key = turn(project(w_key), positions) * HEAD_DIM ** (-0.5)
    value = project(w_value)
    gate = project(w_gate)
    heads = jnp.arange(HEADS, dtype=jnp.float32)
    gamma = 1.0 - 2.0 ** (-5.0 - 5.0 * heads / (HEADS - 1))
    new_state = gamma[None, :, None, None] * state + key[:, :, :, None] * value[:, :, None, :]
    read = jnp.einsum('bhd,bhde->bhe', query, new_state, precision=lax.Precision.HIGHEST)
    read = read * lax.rsqrt(lax.optimization_barrier(jnp.mean(read * read, axis=-1, keepdims=True)) + 1e-06)
    retained = (read * jax.nn.silu(gate)).reshape(rows, HEADS * HEAD_DIM).astype(jnp.bfloat16)
    mixed = (inputs + jnp.dot(retained, w_out, preferred_element_type=jnp.float32)).astype(jnp.bfloat16)
    middle = mixed.astype(jnp.float32)
    scale2 = lax.rsqrt(lax.optimization_barrier(jnp.mean(middle * middle, axis=1)) + 1e-06)
    normed2 = (middle * mlp_gain).astype(jnp.bfloat16)
    upward = jnp.dot(normed2, w_up, preferred_element_type=jnp.float32) * scale2[:, None]
    hidden = jnp.square(jax.nn.relu(upward)).astype(jnp.bfloat16)
    layer_out = (middle + jnp.dot(hidden, w_down, preferred_element_type=jnp.float32)).astype(jnp.bfloat16)
    return (layer_out, new_state)
```

```python
import jax
import jax.numpy as jnp
from jax import lax
from jax.sharding import PartitionSpec as P

D = 4096
HEADS = 16
DIRECT = 8


def turn(values, positions):
    half = values.shape[-1] // 2
    freq = 10000.0 ** (-(jnp.arange(half, dtype=jnp.float32) * 2.0) / values.shape[-1])
    angle = positions.astype(jnp.float32)[:, None, None] * freq[None, None, :]
    cosine = jnp.cos(angle)
    sine = jnp.sin(angle)
    first = values[..., :half]
    second = values[..., half:]
    return jnp.concatenate(
        [first * cosine - second * sine, first * sine + second * cosine], axis=-1
    )


def swap(value, axis, n, step):
    return lax.ppermute(value, axis, [(i, i ^ step) for i in range(n)])


def pieces(value):
    high = lax.reduce_precision(value, 8, 7)
    rest = value - high
    middle = lax.reduce_precision(rest, 8, 7)
    return [p.astype(jnp.bfloat16) for p in (high, middle, rest - middle)]


def scatter_sum(chunk, axis, n):
    me = lax.axis_index(axis)
    mine = chunk(me)
    got = [swap(chunk(me ^ s).astype(jnp.bfloat16), axis, n, s) for s in range(1, n)]
    total = mine
    for g in got:
        total = total + g.astype(jnp.float32)
    return total


def all_sum(value, axis, n):
    sent = value.astype(jnp.bfloat16)
    total = value
    for g in [swap(sent, axis, n, s) for s in range(1, n)]:
        total = total + g.astype(jnp.float32)
    return total


def gather(value, axis, n):
    me = lax.axis_index(axis)
    got = [value] + [swap(value, axis, n, s) for s in range(1, n)]
    out = jnp.zeros((n, *value.shape), value.dtype)
    for s, g in enumerate(got):
        out = lax.dynamic_update_slice_in_dim(out, g[None], me ^ s, 0)
    return out


def make(mesh):
    n_kv, n_tp = mesh.shape["kv"], mesh.shape["tp"]

    def shards(
        tokens, positions, state, norm_gain, w_query, w_key, w_value, w_gate, w_out, mlp_gain, w_up, w_down
    ):
        local_seqs, head_dev, head_size, _ = state.shape
        rows = tokens.shape[0]
        width = head_dev * head_size
        inputs = tokens.astype(jnp.float32)
        squares = jnp.sum(inputs * inputs, axis=1)
        normed = (inputs * norm_gain).astype(jnp.bfloat16)
        terms = jnp.concatenate(
            [
                jnp.dot(normed, weight, preferred_element_type=jnp.float32)
                for weight in (w_query, w_key, w_value, w_gate)
            ]
            + [jnp.broadcast_to(p.astype(jnp.float32)[:, None], (rows, 128)) for p in pieces(squares)],
            axis=1,
        )
        total = scatter_sum(
            lambda i: lax.dynamic_slice_in_dim(terms, i * local_seqs, local_seqs, 0), "kv", n_kv
        )
        total_sq = total[:, 4 * width] + total[:, 4 * width + 128] + total[:, 4 * width + 256]
        scale1 = lax.rsqrt(total_sq / D + 1e-06)
        summed = (total[:, : 4 * width] * scale1[:, None]).reshape(local_seqs, 4, head_dev, head_size)
        query = turn(summed[:, 0], positions)
        key_rows = turn(summed[:, 1], positions) * head_size ** (-0.5)
        value = summed[:, 2]
        gate = summed[:, 3]
        heads = (lax.axis_index("tp") * head_dev + jnp.arange(head_dev)).astype(jnp.float32)
        gamma = 1.0 - 2.0 ** (-5.0 - 5.0 * heads / (HEADS - 1))
        new_state = gamma[None, :, None, None] * state + key_rows[:, :, :, None] * value[:, :, None, :]
        read = jnp.einsum("bhd,bhde->bhe", query, new_state, precision=lax.Precision.HIGHEST)
        read = read * lax.rsqrt(jnp.mean(read * read, axis=-1, keepdims=True) + 1e-06)
        retained = (read * jax.nn.silu(gate)).reshape(local_seqs, width).astype(jnp.bfloat16)
        head_terms = jnp.dot(
            gather(retained, "kv", n_kv).reshape(rows, width), w_out, preferred_element_type=jnp.float32
        )
        mixed = (inputs + all_sum(head_terms, "tp", n_tp)).astype(jnp.bfloat16)
        middle = mixed.astype(jnp.float32)
        squares2 = jnp.sum(middle * middle, axis=1)
        normed2 = (middle * mlp_gain).astype(jnp.bfloat16)
        upward = jnp.dot(normed2, w_up, preferred_element_type=jnp.float32)
        part = upward.shape[1] // n_kv
        extra = jnp.concatenate(
            [jnp.broadcast_to(p.astype(jnp.float32)[:, None], (rows, 128)) for p in pieces(squares2)], axis=1
        )
        total2 = scatter_sum(
            lambda i: jnp.concatenate([lax.dynamic_slice_in_dim(upward, i * part, part, 1), extra], axis=1),
            "kv",
            n_kv,
        )
        total_sq2 = total2[:, part] + total2[:, part + 128] + total2[:, part + 256]
        scale2 = lax.rsqrt(total_sq2 / D + 1e-06)
        hidden = jnp.square(jax.nn.relu(total2[:, :part] * scale2[:, None])).astype(jnp.bfloat16)
        full = gather(hidden, "kv", n_kv).transpose(1, 0, 2).reshape(rows, n_kv * part)
        down_terms = jnp.dot(full, w_down, preferred_element_type=jnp.float32)
        layer_out = (middle + all_sum(down_terms, "tp", n_tp)).astype(jnp.bfloat16)
        return (layer_out, new_state)

    return shards


def solution(mesh):
    return jax.shard_map(
        make(mesh),
        mesh=mesh,
        in_specs=(
            P("grp", "kv"),
            P(("grp", "kv")),
            P(("grp", "kv"), "tp", None, None),
            P("kv"),
            P("kv", "tp"),
            P("kv", "tp"),
            P("kv", "tp"),
            P("kv", "tp"),
            P("tp", "kv"),
            P("kv"),
            P("kv", "tp"),
            P("tp", "kv"),
        ),
        out_specs=(P("grp", "kv"), P(("grp", "kv"), "tp", None, None)),
        check_vma=False,
    )
```

```python
import functools

import jax
import jax.numpy as jnp
from jax import lax
from jax.experimental import pallas as pl
from jax.experimental.pallas import tpu as pltpu
from jax.sharding import PartitionSpec as P

D = 4096
HEADS = 16
DIRECT = 8
LANES = 128
F32, BF16 = jnp.float32, jnp.bfloat16


def turn(values, positions):
    half = values.shape[-1] // 2
    freq = 10000.0 ** (-(jnp.arange(half, dtype=jnp.float32) * 2.0) / values.shape[-1])
    angle = positions.astype(jnp.float32)[:, None, None] * freq[None, None, :]
    cosine = jnp.cos(angle)
    sine = jnp.sin(angle)
    first = values[..., :half]
    second = values[..., half:]
    return jnp.concatenate(
        [first * cosine - second * sine, first * sine + second * cosine], axis=-1
    )


def shards_large(
    tokens,
    positions,
    state,
    norm_gain,
    w_query,
    w_key,
    w_value,
    w_gate,
    w_out,
    mlp_gain,
    w_up,
    w_down,
):
    local_seqs, head_dev, head_size, _ = state.shape
    inputs = tokens.astype(jnp.float32)
    squares = jnp.sum(inputs * inputs, axis=1)
    normed = (inputs * norm_gain).astype(jnp.bfloat16)
    terms = jnp.stack(
        [
            jnp.dot(normed, weight, preferred_element_type=jnp.float32)
            for weight in (w_query, w_key, w_value, w_gate)
        ],
        axis=1,
    )
    summed, total_sq = (
        lax.psum_scatter(terms, "kv", scatter_dimension=0, tiled=True),
        lax.psum_scatter(squares, "kv", scatter_dimension=0, tiled=True),
    )
    scale1 = lax.rsqrt(total_sq / D + 1e-06)
    summed = (summed * scale1[:, None, None]).reshape(local_seqs, 4, head_dev, head_size)
    query = turn(summed[:, 0], positions)
    key_rows = turn(summed[:, 1], positions) * head_size ** (-0.5)
    value = summed[:, 2]
    gate = summed[:, 3]
    heads = (lax.axis_index("tp") * head_dev + jnp.arange(head_dev)).astype(jnp.float32)
    gamma = 1.0 - 2.0 ** (-5.0 - 5.0 * heads / (HEADS - 1))
    new_state = gamma[None, :, None, None] * state + key_rows[:, :, :, None] * value[:, :, None, :]
    read = jnp.einsum("bhd,bhde->bhe", query, new_state, precision=lax.Precision.HIGHEST)
    read = read * lax.rsqrt(jnp.mean(read * read, axis=-1, keepdims=True) + 1e-06)
    retained = (
        (read * jax.nn.silu(gate)).reshape(local_seqs, head_dev * head_size).astype(jnp.bfloat16)
    )
    head_terms = jnp.dot(
        lax.all_gather(retained, "kv", axis=0, tiled=True),
        w_out,
        preferred_element_type=jnp.float32,
    )
    mixed = (inputs + lax.psum(head_terms, "tp")).astype(jnp.bfloat16)
    middle = mixed.astype(jnp.float32)
    squares2 = jnp.sum(middle * middle, axis=1)
    normed2 = (middle * mlp_gain).astype(jnp.bfloat16)
    upward = jnp.dot(normed2, w_up, preferred_element_type=jnp.float32)
    up_full, total_sq2 = lax.psum((upward, squares2), "kv")
    scale2 = lax.rsqrt(total_sq2 / D + 1e-06)
    hidden = jnp.square(jax.nn.relu(up_full * scale2[:, None])).astype(jnp.bfloat16)
    down_terms = jnp.dot(hidden, w_down, preferred_element_type=jnp.float32)
    layer_out = (middle + lax.psum(down_terms, "tp")).astype(jnp.bfloat16)
    return (layer_out, new_state)


def swap(value, axis, n, step):
    return lax.ppermute(value, axis, [(i, i ^ step) for i in range(n)])


def pieces(value):
    high = value.astype(BF16).astype(F32)
    rest = value - high
    middle = rest.astype(BF16).astype(F32)
    return high, middle, rest - middle


def reorder(n, values):
    me = lax.axis_index("kv")
    rows = values.shape[0]
    block = rows // n
    to = lax.broadcasted_iota(jnp.int32, (rows, rows), 0)
    of = lax.broadcasted_iota(jnp.int32, (rows, rows), 1)
    hot = ((to // block) ^ me) * block + to % block == of
    return jnp.dot(hot.astype(F32).astype(BF16), values, preferred_element_type=F32)


def project_kernel(n, x_ref, gain_ref, *refs):
    weights, (own_ref, *sent), (held, sems) = refs[:4], refs[4 : 4 + n], refs[4 + n :]
    copies = []
    depth = x_ref.shape[1]
    half = depth // 2
    for i, w in enumerate(weights):
        for j in range(2):
            part = pl.ds(j * half, half)
            copies.append(pltpu.make_async_copy(w.at[part], held.at[i, part], sems.at[i, j]))
    for copy in copies:
        copy.start()
    x = reorder(n, x_ref[...])
    squares = jnp.sum(x * x, axis=1, keepdims=True)
    normed = (x * gain_ref[...]).astype(BF16)
    rows, width = x.shape[0], held.shape[2]
    block = rows // n
    split = [jnp.broadcast_to(p, (rows, LANES)) for p in pieces(squares)]
    split.append(jnp.zeros((rows, LANES), F32))
    outs = (own_ref, *sent)
    for i in range(4):
        total = None
        for j in range(2):
            copies[2 * i + j].wait()
            part = slice(j * half, (j + 1) * half)
            term = jnp.dot(normed[:, part], held[i, part], preferred_element_type=F32)
            total = term if total is None else total + term
        for s, out in enumerate(outs):
            here = slice(i * block, (i + 1) * block)
            out[here, :width] = total[s * block : (s + 1) * block].astype(out.dtype)
            out[here, width:] = split[i][s * block : (s + 1) * block].astype(out.dtype)


def retain_kernel(n, own_ref, *refs):
    got, (cos_ref, sin_ref, gamma_ref, state_ref, new_ref, kept_ref) = refs[: n - 1], refs[n - 1 :]
    block, head_dev, size, _ = state_ref.shape
    width = head_dev * size
    total = own_ref[...]
    for g in got:
        total = total + g[...].astype(F32)
    sq = total[:, width : width + 1]
    total_sq = sq[:block] + sq[block : 2 * block] + sq[2 * block : 3 * block]
    scale = lax.rsqrt(total_sq / D + 1e-06)
    query, key, value, gate = (total[i * block : (i + 1) * block, :width] * scale for i in range(4))
    cos, sin = cos_ref[...], sin_ref[...]
    gate = gate / (1.0 + jnp.exp(-gate))
    for h in range(head_dev):
        at = slice(h * size, (h + 1) * size)
        q, k = query[:, at], key[:, at]
        q = q * cos + pltpu.roll(q, size // 2, 1) * sin
        k = (k * cos + pltpu.roll(k, size // 2, 1) * sin) * size ** (-0.5)
        columns = jnp.concatenate([q, k], axis=0).T
        v = value[:, at]
        gamma = gamma_ref[h : h + 1, :]
        reads = []
        for b in range(block):
            new = gamma * state_ref[b, h] + columns[:, block + b : block + b + 1] * v[b : b + 1]
            new_ref[b, h] = new
            reads.append(jnp.sum(columns[:, b : b + 1] * new, axis=0, keepdims=True))
        read = jnp.concatenate(reads, axis=0)
        read = read * lax.rsqrt(jnp.mean(read * read, axis=1, keepdims=True) + 1e-06)
        kept_ref[:, at] = (read * gate[:, at]).astype(BF16)


def out_kernel(n, *refs):
    parts, (w_ref, own_ref, sent_ref) = refs[:n], refs[n:]
    kept = jnp.concatenate([p[...].astype(F32) for p in parts], axis=0).astype(BF16)
    kept = reorder(n, kept).astype(BF16)
    terms = jnp.dot(kept, w_ref[...], preferred_element_type=F32)
    own_ref[...] = terms
    sent_ref[...] = terms.astype(BF16)


def up_kernel(n_tp, n, x_ref, gain_ref, w_ref, own_ref, *refs):
    got, (mixed_ref, total_ref, *sent) = refs[: n_tp - 1], refs[n_tp - 1 :]
    total = own_ref[...]
    for g in got:
        total = total + g[...].astype(F32)
    mixed = (x_ref[...].astype(F32) + total).astype(BF16)
    mixed_ref[...] = mixed
    middle = mixed.astype(F32)
    normed = (middle * gain_ref[...]).astype(BF16)
    rows = middle.shape[0]
    high, mid, low = pieces(jnp.sum(middle * middle, axis=1, keepdims=True))
    lane = lax.broadcasted_iota(jnp.int32, (rows, LANES), 1)
    split = jnp.where(lane == 0, high, jnp.where(lane == 1, mid, jnp.where(lane == 2, low, 0.0)))
    part = w_ref.shape[1] // n
    me = lax.axis_index("kv")
    for s in reversed(range(n)):
        at = pl.ds(pl.multiple_of((me ^ s) * part, part), part)
        out = sent[s - 1] if s else total_ref
        out[:, :part] = jnp.dot(normed, w_ref[:, at], preferred_element_type=F32).astype(out.dtype)
        out[:, part:] = split.astype(out.dtype)


def hidden_kernel(own_ref, *refs):
    *got, out_ref = refs
    total = own_ref[...]
    for g in got:
        total = total + g[...].astype(F32)
    part = out_ref.shape[1]
    sq = total[:, part : part + 1] + total[:, part + 1 : part + 2] + total[:, part + 2 : part + 3]
    scale = lax.rsqrt(sq / D + 1e-06)
    out_ref[...] = jnp.square(jnp.maximum(total[:, :part] * scale, 0.0)).astype(BF16)


def down_kernel(n, *refs):
    parts, (w_ref, own_ref, sent_ref) = refs[:n], refs[n:]
    me = lax.axis_index("kv")
    part = w_ref.shape[0] // n
    total = None
    for s, p in enumerate(parts):
        at = pl.ds(pl.multiple_of((me ^ s) * part, part), part)
        term = jnp.dot(p[...], w_ref[at, :], preferred_element_type=F32)
        total = term if total is None else total + term
    own_ref[...] = total
    sent_ref[...] = total.astype(BF16)


def final_kernel(mixed_ref, own_ref, *refs):
    *got, out_ref = refs
    total = own_ref[...]
    for g in got:
        total = total + g[...].astype(F32)
    out_ref[...] = (mixed_ref[...].astype(F32) + total).astype(BF16)


VMEM = pl.BlockSpec(memory_space=pltpu.VMEM)
HBM = pl.BlockSpec(memory_space=pltpu.HBM)


def call(kernel, name, outs, *args, specs=None, scratch=(), limit=8):
    return pl.pallas_call(
        kernel,
        name=name,
        out_shape=[jax.ShapeDtypeStruct(*o) for o in outs],
        in_specs=specs or [VMEM] * len(args),
        out_specs=[VMEM] * len(outs),
        scratch_shapes=scratch,
        compiler_params=pltpu.CompilerParams(vmem_limit_bytes=limit << 20),
    )(*args)


def near(value):
    return pltpu.with_memory_space_constraint(value, pltpu.VMEM)


def make_direct(n, n_tp):
    def shards(
        tokens, positions, state, norm_gain, w_query, w_key, w_value, w_gate, w_out, mlp_gain, w_up, w_down
    ):
        block, head_dev, size, _ = state.shape
        rows, depth = tokens.shape
        width = head_dev * size
        wide = width + LANES
        own, *sent = call(
            functools.partial(project_kernel, n),
            "project",
            [((4 * block, wide), F32)] + [((4 * block, wide), BF16)] * (n - 1),
            tokens,
            norm_gain[None],
            w_query,
            w_key,
            w_value,
            w_gate,
            specs=[VMEM, VMEM] + [HBM] * 4,
            scratch=[pltpu.VMEM((4, depth, width), BF16), pltpu.SemaphoreType.DMA((4, 2))],
            limit=8,
        )
        got = [swap(v, "kv", n, s) for s, v in enumerate(sent, 1)]
        half = size // 2
        freq = 10000.0 ** (-(jnp.arange(half, dtype=F32) * 2.0) / size)
        angle = positions.astype(F32)[:, None] * freq[None, :]
        cosine, sine = jnp.cos(angle), jnp.sin(angle)
        cosine = jnp.concatenate([cosine, cosine], axis=1)
        sine = jnp.concatenate([-sine, sine], axis=1)
        heads = (lax.axis_index("tp") * head_dev + jnp.arange(head_dev)).astype(F32)
        gamma = 1.0 - 2.0 ** (-5.0 - 5.0 * heads / (HEADS - 1))
        gamma = jnp.broadcast_to(gamma[:, None], (head_dev, size))
        new_state, kept = call(
            functools.partial(retain_kernel, n),
            "retain",
            [(state.shape, F32), ((block, width), BF16)],
            own,
            *got,
            cosine,
            sine,
            gamma,
            near(state),
        )
        kept = [kept] + [swap(kept, "kv", n, s) for s in range(1, n)]
        own, sent = call(
            functools.partial(out_kernel, n),
            "out",
            [((rows, depth), F32), ((rows, depth), BF16)],
            *kept,
            near(w_out),
        )
        got = [swap(sent, "tp", n_tp, s) for s in range(1, n_tp)]
        part = w_up.shape[1] // n
        mixed, own, *sent = call(
            functools.partial(up_kernel, n_tp, n),
            "up",
            [((rows, depth), BF16), ((rows, part + LANES), F32)] + [((rows, part + LANES), BF16)] * (n - 1),
            tokens,
            mlp_gain[None],
            near(w_up),
            own,
            *got,
        )
        got = [swap(v, "kv", n, s) for s, v in enumerate(sent, 1)]
        (hidden,) = call(hidden_kernel, "hidden", [((rows, part), BF16)], own, *got)
        hidden = [hidden] + [swap(hidden, "kv", n, s) for s in range(1, n)]
        own, sent = call(
            functools.partial(down_kernel, n),
            "down",
            [((rows, depth), F32), ((rows, depth), BF16)],
            *hidden,
            near(w_down),
        )
        got = [swap(sent, "tp", n_tp, s) for s in range(1, n_tp)]
        (layer_out,) = call(final_kernel, "final", [((rows, depth), BF16)], mixed, own, *got)
        return (layer_out, new_state)

    return shards


def solution(mesh):
    n_kv, n_tp = mesh.shape["kv"], mesh.shape["tp"]
    direct = all(n <= DIRECT and n & (n - 1) == 0 for n in (n_kv, n_tp))
    return jax.shard_map(
        make_direct(n_kv, n_tp) if direct else shards_large,
        mesh=mesh,
        in_specs=(
            P("grp", "kv"),
            P(("grp", "kv")),
            P(("grp", "kv"), "tp", None, None),
            P("kv"),
            P("kv", "tp"),
            P("kv", "tp"),
            P("kv", "tp"),
            P("kv", "tp"),
            P("tp", "kv"),
            P("kv"),
            P("kv", "tp"),
            P("tp", "kv"),
        ),
        out_specs=(P("grp", "kv"), P(("grp", "kv"), "tp", None, None)),
        check_vma=False,
    )
```

```python
import functools

import jax
import jax.numpy as jnp
from jax import lax
from jax.experimental import pallas as pl
from jax.experimental.pallas import tpu as pltpu
from jax.sharding import PartitionSpec as P

D = 4096
HEADS = 16
DIRECT = 8
LANES = 128
RATE = 1 << 36
F32, BF16 = jnp.float32, jnp.bfloat16


def turn(values, positions):
    half = values.shape[-1] // 2
    freq = 10000.0 ** (-(jnp.arange(half, dtype=jnp.float32) * 2.0) / values.shape[-1])
    angle = positions.astype(jnp.float32)[:, None, None] * freq[None, None, :]
    cosine = jnp.cos(angle)
    sine = jnp.sin(angle)
    first = values[..., :half]
    second = values[..., half:]
    return jnp.concatenate(
        [first * cosine - second * sine, first * sine + second * cosine], axis=-1
    )


def shards_large(
    tokens,
    positions,
    state,
    norm_gain,
    w_query,
    w_key,
    w_value,
    w_gate,
    w_out,
    mlp_gain,
    w_up,
    w_down,
):
    local_seqs, head_dev, head_size, _ = state.shape
    inputs = tokens.astype(jnp.float32)
    squares = jnp.sum(inputs * inputs, axis=1)
    normed = (inputs * norm_gain).astype(jnp.bfloat16)
    terms = jnp.stack(
        [
            jnp.dot(normed, weight, preferred_element_type=jnp.float32)
            for weight in (w_query, w_key, w_value, w_gate)
        ],
        axis=1,
    )
    summed, total_sq = (
        lax.psum_scatter(terms, "kv", scatter_dimension=0, tiled=True),
        lax.psum_scatter(squares, "kv", scatter_dimension=0, tiled=True),
    )
    scale1 = lax.rsqrt(total_sq / D + 1e-06)
    summed = (summed * scale1[:, None, None]).reshape(local_seqs, 4, head_dev, head_size)
    query = turn(summed[:, 0], positions)
    key_rows = turn(summed[:, 1], positions) * head_size ** (-0.5)
    value = summed[:, 2]
    gate = summed[:, 3]
    heads = (lax.axis_index("tp") * head_dev + jnp.arange(head_dev)).astype(jnp.float32)
    gamma = 1.0 - 2.0 ** (-5.0 - 5.0 * heads / (HEADS - 1))
    new_state = gamma[None, :, None, None] * state + key_rows[:, :, :, None] * value[:, :, None, :]
    read = jnp.einsum("bhd,bhde->bhe", query, new_state, precision=lax.Precision.HIGHEST)
    read = read * lax.rsqrt(jnp.mean(read * read, axis=-1, keepdims=True) + 1e-06)
    retained = (
        (read * jax.nn.silu(gate)).reshape(local_seqs, head_dev * head_size).astype(jnp.bfloat16)
    )
    head_terms = jnp.dot(
        lax.all_gather(retained, "kv", axis=0, tiled=True),
        w_out,
        preferred_element_type=jnp.float32,
    )
    mixed = (inputs + lax.psum(head_terms, "tp")).astype(jnp.bfloat16)
    middle = mixed.astype(jnp.float32)
    squares2 = jnp.sum(middle * middle, axis=1)
    normed2 = (middle * mlp_gain).astype(jnp.bfloat16)
    upward = jnp.dot(normed2, w_up, preferred_element_type=jnp.float32)
    up_full, total_sq2 = lax.psum((upward, squares2), "kv")
    scale2 = lax.rsqrt(total_sq2 / D + 1e-06)
    hidden = jnp.square(jax.nn.relu(up_full * scale2[:, None])).astype(jnp.bfloat16)
    down_terms = jnp.dot(hidden, w_down, preferred_element_type=jnp.float32)
    layer_out = (middle + lax.psum(down_terms, "tp")).astype(jnp.bfloat16)
    return (layer_out, new_state)


def swap(value, axis, n, step):
    return lax.ppermute(value, axis, [(i, i ^ step) for i in range(n)])


def pieces(value):
    high = value.astype(BF16).astype(F32)
    rest = value - high
    middle = rest.astype(BF16).astype(F32)
    return high, middle, rest - middle


def reorder(n, values):
    me = lax.axis_index("kv")
    rows = values.shape[0]
    block = rows // n
    to = lax.broadcasted_iota(jnp.int32, (rows, rows), 0)
    of = lax.broadcasted_iota(jnp.int32, (rows, rows), 1)
    hot = ((to // block) ^ me) * block + to % block == of
    return jnp.dot(hot.astype(F32).astype(BF16), values, preferred_element_type=F32)


def project_kernel(n, x_hbm, gain_hbm, *refs):
    weights, (own_ref, *sent), (x_ref, gain_ref, held, sems, small) = refs[:4], refs[4 : 4 + n], refs[4 + n :]
    first = [
        pltpu.make_async_copy(x_hbm, x_ref, small.at[0]),
        pltpu.make_async_copy(gain_hbm, gain_ref, small.at[1]),
    ]
    depth = x_ref.shape[1]
    half = depth // 2
    copies = []
    for i, w in enumerate(weights):
        for j in range(2):
            part = pl.ds(j * half, half)
            copies.append(pltpu.make_async_copy(w.at[part], held.at[i, part], sems.at[i, j]))
    for copy in first + copies:
        copy.start()
    first[0].wait()
    x = reorder(n, x_ref[...])
    squares = jnp.sum(x * x, axis=1, keepdims=True)
    first[1].wait()
    normed = (x * gain_ref[...]).astype(BF16)
    rows, width = x.shape[0], held.shape[2]
    block = rows // n
    split = [jnp.broadcast_to(p, (rows, LANES)) for p in pieces(squares)]
    split.append(jnp.zeros((rows, LANES), F32))
    outs = (own_ref, *sent)
    for i in range(4):
        total = None
        for j in range(2):
            copies[2 * i + j].wait()
            part = slice(j * half, (j + 1) * half)
            term = jnp.dot(normed[:, part], held[i, part], preferred_element_type=F32)
            total = term if total is None else total + term
        for s, out in enumerate(outs):
            here = slice(i * block, (i + 1) * block)
            out[here, :width] = total[s * block : (s + 1) * block].astype(out.dtype)
            out[here, width:] = split[i][s * block : (s + 1) * block].astype(out.dtype)


def read_kernel(n, own_ref, *refs):
    got, (cos_ref, sin_ref, gamma_ref, state_ref, kept_ref, key_ref, value_ref) = refs[: n - 1], refs[n - 1 :]
    block, head_dev, size, _ = state_ref.shape
    width = head_dev * size
    total = own_ref[...]
    for g in got:
        total = total + g[...].astype(F32)
    sq = total[:, width : width + 1]
    total_sq = sq[:block] + sq[block : 2 * block] + sq[2 * block : 3 * block]
    scale = lax.rsqrt(total_sq / D + 1e-06)
    query, key, value, gate = (total[i * block : (i + 1) * block, :width] * scale for i in range(4))
    value_ref[...] = value
    cos, sin = cos_ref[...], sin_ref[...]
    gate = gate / (1.0 + jnp.exp(-gate))
    for h in range(head_dev):
        at = slice(h * size, (h + 1) * size)
        q, k = query[:, at], key[:, at]
        q = q * cos + pltpu.roll(q, size // 2, 1) * sin
        k = (k * cos + pltpu.roll(k, size // 2, 1) * sin) * size ** (-0.5)
        key_ref[:, at] = k
        columns = jnp.concatenate([q, k], axis=0).T
        reads = []
        for b in range(block):
            reads.append(jnp.sum(columns[:, b : b + 1] * state_ref[b, h], axis=0, keepdims=True))
        match = jnp.sum(q * k, axis=1, keepdims=True)
        read = gamma_ref[h : h + 1, :] * jnp.concatenate(reads, axis=0) + match * value[:, at]
        read = read * lax.rsqrt(jnp.mean(read * read, axis=1, keepdims=True) + 1e-06)
        kept_ref[:, at] = (read * gate[:, at]).astype(BF16)


def update_kernel(key_ref, value_ref, gamma_ref, after_ref, state_ref, new_hbm, new_ref, sems):
    del after_ref
    block, head_dev, size, _ = state_ref.shape
    copies = []
    for h in range(head_dev):
        at = slice(h * size, (h + 1) * size)
        k = key_ref[:, at]
        columns = jnp.concatenate([k, k], axis=0).T
        gamma = gamma_ref[h : h + 1, :]
        for b in range(block):
            new_ref[b, h] = gamma * state_ref[b, h] + columns[:, b : b + 1] * value_ref[b : b + 1, at]
            copies.append(pltpu.make_async_copy(new_ref.at[b, h], new_hbm.at[b, h], sems.at[b, h]))
            copies[-1].start()
    for copy in copies:
        copy.wait()


def out_kernel(n, *refs):
    parts, (w_ref, own_ref, sent_ref) = refs[:n], refs[n:]
    kept = jnp.concatenate([p[...].astype(F32) for p in parts], axis=0).astype(BF16)
    kept = reorder(n, kept).astype(BF16)
    terms = jnp.dot(kept, w_ref[...], preferred_element_type=F32)
    own_ref[...] = terms
    sent_ref[...] = terms.astype(BF16)


def up_kernel(n_tp, n, x_ref, gain_ref, w_ref, own_ref, *refs):
    got, (mixed_ref, normed_ref, split_ref, *sent) = refs[: n_tp - 1], refs[n_tp - 1 :]
    total = own_ref[...]
    for g in got:
        total = total + g[...].astype(F32)
    mixed = (x_ref[...].astype(F32) + total).astype(BF16)
    mixed_ref[...] = mixed
    middle = mixed.astype(F32)
    normed = (middle * gain_ref[...]).astype(BF16)
    normed_ref[...] = normed
    rows = middle.shape[0]
    high, mid, low = pieces(jnp.sum(middle * middle, axis=1, keepdims=True))
    lane = lax.broadcasted_iota(jnp.int32, (rows, LANES), 1)
    split = jnp.where(lane == 0, high, jnp.where(lane == 1, mid, jnp.where(lane == 2, low, 0.0)))
    split_ref[...] = split
    part = w_ref.shape[1] // n
    me = lax.axis_index("kv")
    for s in reversed(range(1, n)):
        at = pl.ds(pl.multiple_of((me ^ s) * part, part), part)
        out = sent[s - 1]
        out[:, :part] = jnp.dot(normed, w_ref[:, at], preferred_element_type=F32).astype(out.dtype)
        out[:, part:] = split.astype(out.dtype)


def up_own_kernel(n, normed_ref, w_ref, out_ref):
    part = w_ref.shape[1] // n
    at = pl.ds(pl.multiple_of(lax.axis_index("kv") * part, part), part)
    out_ref[...] = jnp.dot(normed_ref[...], w_ref[:, at], preferred_element_type=F32)


def hidden_kernel(own_ref, split_ref, *refs):
    *got, out_ref = refs
    part = out_ref.shape[1]
    total, split = own_ref[...], split_ref[...]
    for g in got:
        total = total + g[:, :part].astype(F32)
        split = split + g[:, part:].astype(F32)
    sq = split[:, 0:1] + split[:, 1:2] + split[:, 2:3]
    scale = lax.rsqrt(sq / D + 1e-06)
    out_ref[...] = jnp.square(jnp.maximum(total * scale, 0.0)).astype(BF16)


def down_own_kernel(n, hidden_ref, w_ref, out_ref):
    part = w_ref.shape[0] // n
    at = pl.ds(pl.multiple_of(lax.axis_index("kv") * part, part), part)
    out_ref[...] = jnp.dot(hidden_ref[...], w_ref[at, :], preferred_element_type=F32)


def down_kernel(n, start_ref, *refs):
    parts, (w_ref, own_ref, sent_ref) = refs[: n - 1], refs[n - 1 :]
    me = lax.axis_index("kv")
    part = w_ref.shape[0] // n
    total = start_ref[...]
    for s, p in enumerate(parts, 1):
        at = pl.ds(pl.multiple_of((me ^ s) * part, part), part)
        total = total + jnp.dot(p[...], w_ref[at, :], preferred_element_type=F32)
    own_ref[...] = total
    sent_ref[...] = total.astype(BF16)


def final_kernel(mixed_ref, own_ref, *refs):
    *got, out_ref = refs
    total = own_ref[...]
    for g in got:
        total = total + g[...].astype(F32)
    out_ref[...] = (mixed_ref[...].astype(F32) + total).astype(BF16)


VMEM = pl.BlockSpec(memory_space=pltpu.VMEM)
HBM = pl.BlockSpec(memory_space=pltpu.HBM)


def call(kernel, name, outs, *args, specs=None, out_specs=None, scratch=(), limit=8, us=1):
    return pl.pallas_call(
        kernel,
        name=name,
        out_shape=[jax.ShapeDtypeStruct(*o) for o in outs],
        in_specs=specs or [VMEM] * len(args),
        out_specs=out_specs or [VMEM] * len(outs),
        scratch_shapes=scratch,
        compiler_params=pltpu.CompilerParams(vmem_limit_bytes=limit << 20),
        cost_estimate=pl.CostEstimate(flops=int(us * RATE), bytes_accessed=0, transcendentals=0),
    )(*args)


def far(value):
    return pltpu.with_memory_space_constraint(value, pltpu.HBM)


def near(value):
    return pltpu.with_memory_space_constraint(value, pltpu.VMEM)


def make_direct(n, n_tp):
    def shards(
        tokens, positions, state, norm_gain, w_query, w_key, w_value, w_gate, w_out, mlp_gain, w_up, w_down
    ):
        block, head_dev, size, _ = state.shape
        rows, depth = tokens.shape
        width = head_dev * size
        wide = width + LANES
        own, *sent = call(
            functools.partial(project_kernel, n),
            "project",
            [((4 * block, wide), F32)] + [((4 * block, wide), BF16)] * (n - 1),
            far(tokens),
            far(norm_gain[None]),
            far(w_query),
            far(w_key),
            far(w_value),
            far(w_gate),
            specs=[HBM] * 6,
            scratch=[
                pltpu.VMEM((rows, depth), BF16),
                pltpu.VMEM((1, depth), F32),
                pltpu.VMEM((4, depth, width), BF16),
                pltpu.SemaphoreType.DMA((4, 2)),
                pltpu.SemaphoreType.DMA((2,)),
            ],
            us=2,
        )
        got = [swap(v, "kv", n, s) for s, v in enumerate(sent, 1)]
        half = size // 2
        freq = 10000.0 ** (-(jnp.arange(half, dtype=F32) * 2.0) / size)
        angle = positions.astype(F32)[:, None] * freq[None, :]
        cosine, sine = jnp.cos(angle), jnp.sin(angle)
        cosine = jnp.concatenate([cosine, cosine], axis=1)
        sine = jnp.concatenate([-sine, sine], axis=1)
        heads = (lax.axis_index("tp") * head_dev + jnp.arange(head_dev)).astype(F32)
        gamma = 1.0 - 2.0 ** (-5.0 - 5.0 * heads / (HEADS - 1))
        gamma = jnp.broadcast_to(gamma[:, None], (head_dev, size))
        state = near(state)
        kept, key, value = call(
            functools.partial(read_kernel, n),
            "read",
            [((block, width), BF16), ((block, width), F32), ((block, width), F32)],
            own,
            *got,
            cosine,
            sine,
            gamma,
            state,
            us=1,
        )
        kept = [kept] + [swap(kept, "kv", n, s) for s in range(1, n)]
        own, sent = call(
            functools.partial(out_kernel, n),
            "out",
            [((rows, depth), F32), ((rows, depth), BF16)],
            *kept,
            near(w_out),
        )
        got = [swap(sent, "tp", n_tp, s) for s in range(1, n_tp)]
        part = w_up.shape[1] // n
        w_up = near(w_up)
        mixed, normed, split, *sent = call(
            functools.partial(up_kernel, n_tp, n),
            "up",
            [((rows, depth), BF16), ((rows, depth), BF16), ((rows, LANES), F32)]
            + [((rows, part + LANES), BF16)] * (n - 1),
            tokens,
            mlp_gain[None],
            w_up,
            own,
            *got,
        )
        got = [swap(v, "kv", n, s) for s, v in enumerate(sent, 1)]
        (new_state,) = call(
            update_kernel,
            "update",
            [(state.shape, F32)],
            key,
            value,
            gamma,
            split,
            state,
            out_specs=[HBM],
            scratch=[pltpu.VMEM(state.shape, F32), pltpu.SemaphoreType.DMA((block, head_dev))],
        )
        (own,) = call(
            functools.partial(up_own_kernel, n), "up_own", [((rows, part), F32)], normed, w_up
        )
        (hidden,) = call(hidden_kernel, "hidden", [((rows, part), BF16)], own, split, *got)
        got = [swap(hidden, "kv", n, s) for s in range(1, n)]
        w_down = near(w_down)
        (own,) = call(
            functools.partial(down_own_kernel, n), "down_own", [((rows, depth), F32)], hidden, w_down
        )
        own, sent = call(
            functools.partial(down_kernel, n),
            "down",
            [((rows, depth), F32), ((rows, depth), BF16)],
            own,
            *got,
            w_down,
        )
        got = [swap(sent, "tp", n_tp, s) for s in range(1, n_tp)]
        (layer_out,) = call(final_kernel, "final", [((rows, depth), BF16)], mixed, own, *got)
        return (layer_out, new_state)

    return shards


def solution(mesh):
    n_kv, n_tp = mesh.shape["kv"], mesh.shape["tp"]
    direct = all(n <= DIRECT and n & (n - 1) == 0 for n in (n_kv, n_tp))
    return jax.shard_map(
        make_direct(n_kv, n_tp) if direct else shards_large,
        mesh=mesh,
        in_specs=(
            P("grp", "kv"),
            P(("grp", "kv")),
            P(("grp", "kv"), "tp", None, None),
            P("kv"),
            P("kv", "tp"),
            P("kv", "tp"),
            P("kv", "tp"),
            P("kv", "tp"),
            P("tp", "kv"),
            P("kv"),
            P("kv", "tp"),
            P("tp", "kv"),
        ),
        out_specs=(P("grp", "kv"), P(("grp", "kv"), "tp", None, None)),
        check_vma=False,
    )
```

```python
import functools

import jax
import jax.numpy as jnp
from jax import lax
from jax.experimental import pallas as pl
from jax.experimental.pallas import tpu as pltpu
from jax.sharding import PartitionSpec as P

D = 4096
HEADS = 16
DIRECT = 8
LANES = 128
RATE = 1 << 36
F32, BF16 = jnp.float32, jnp.bfloat16


def turn(values, positions):
    half = values.shape[-1] // 2
    freq = 10000.0 ** (-(jnp.arange(half, dtype=jnp.float32) * 2.0) / values.shape[-1])
    angle = positions.astype(jnp.float32)[:, None, None] * freq[None, None, :]
    cosine = jnp.cos(angle)
    sine = jnp.sin(angle)
    first = values[..., :half]
    second = values[..., half:]
    return jnp.concatenate(
        [first * cosine - second * sine, first * sine + second * cosine], axis=-1
    )


def shards_large(
    tokens,
    positions,
    state,
    norm_gain,
    w_query,
    w_key,
    w_value,
    w_gate,
    w_out,
    mlp_gain,
    w_up,
    w_down,
):
    local_seqs, head_dev, head_size, _ = state.shape
    inputs = tokens.astype(jnp.float32)
    squares = jnp.sum(inputs * inputs, axis=1)
    normed = (inputs * norm_gain).astype(jnp.bfloat16)
    terms = jnp.stack(
        [
            jnp.dot(normed, weight, preferred_element_type=jnp.float32)
            for weight in (w_query, w_key, w_value, w_gate)
        ],
        axis=1,
    )
    summed, total_sq = (
        lax.psum_scatter(terms, "kv", scatter_dimension=0, tiled=True),
        lax.psum_scatter(squares, "kv", scatter_dimension=0, tiled=True),
    )
    scale1 = lax.rsqrt(total_sq / D + 1e-06)
    summed = (summed * scale1[:, None, None]).reshape(local_seqs, 4, head_dev, head_size)
    query = turn(summed[:, 0], positions)
    key_rows = turn(summed[:, 1], positions) * head_size ** (-0.5)
    value = summed[:, 2]
    gate = summed[:, 3]
    heads = (lax.axis_index("tp") * head_dev + jnp.arange(head_dev)).astype(jnp.float32)
    gamma = 1.0 - 2.0 ** (-5.0 - 5.0 * heads / (HEADS - 1))
    new_state = gamma[None, :, None, None] * state + key_rows[:, :, :, None] * value[:, :, None, :]
    read = jnp.einsum("bhd,bhde->bhe", query, new_state, precision=lax.Precision.HIGHEST)
    read = read * lax.rsqrt(jnp.mean(read * read, axis=-1, keepdims=True) + 1e-06)
    retained = (
        (read * jax.nn.silu(gate)).reshape(local_seqs, head_dev * head_size).astype(jnp.bfloat16)
    )
    head_terms = jnp.dot(
        lax.all_gather(retained, "kv", axis=0, tiled=True),
        w_out,
        preferred_element_type=jnp.float32,
    )
    mixed = (inputs + lax.psum(head_terms, "tp")).astype(jnp.bfloat16)
    middle = mixed.astype(jnp.float32)
    squares2 = jnp.sum(middle * middle, axis=1)
    normed2 = (middle * mlp_gain).astype(jnp.bfloat16)
    upward = jnp.dot(normed2, w_up, preferred_element_type=jnp.float32)
    up_full, total_sq2 = lax.psum((upward, squares2), "kv")
    scale2 = lax.rsqrt(total_sq2 / D + 1e-06)
    hidden = jnp.square(jax.nn.relu(up_full * scale2[:, None])).astype(jnp.bfloat16)
    down_terms = jnp.dot(hidden, w_down, preferred_element_type=jnp.float32)
    layer_out = (middle + lax.psum(down_terms, "tp")).astype(jnp.bfloat16)
    return (layer_out, new_state)


def swap(value, axis, n, step):
    return lax.ppermute(value, axis, [(i, i ^ step) for i in range(n)])


def pieces(value):
    high = value.astype(BF16).astype(F32)
    rest = value - high
    middle = rest.astype(BF16).astype(F32)
    return high, middle, rest - middle


def reorder(n, values):
    me = lax.axis_index("kv")
    rows = values.shape[0]
    block = rows // n
    to = lax.broadcasted_iota(jnp.int32, (rows, rows), 0)
    of = lax.broadcasted_iota(jnp.int32, (rows, rows), 1)
    hot = ((to // block) ^ me) * block + to % block == of
    return jnp.dot(hot.astype(F32).astype(BF16), values, preferred_element_type=F32)


def project_kernel(n, x_hbm, gain_hbm, *refs):
    weights, (own_ref, *sent), (x_ref, gain_ref, held, sems, small) = refs[:4], refs[4 : 4 + n], refs[4 + n :]
    first = [
        pltpu.make_async_copy(x_hbm, x_ref, small.at[0]),
        pltpu.make_async_copy(gain_hbm, gain_ref, small.at[1]),
    ]
    depth = x_ref.shape[1]
    half = depth // 2
    copies = []
    for i, w in enumerate(weights):
        for j in range(2):
            part = pl.ds(j * half, half)
            copies.append(pltpu.make_async_copy(w.at[part], held.at[i, part], sems.at[i, j]))
    for copy in first + copies:
        copy.start()
    first[0].wait()
    x = reorder(n, x_ref[...])
    squares = jnp.sum(x * x, axis=1, keepdims=True)
    first[1].wait()
    normed = (x * gain_ref[...]).astype(BF16)
    rows, width = x.shape[0], held.shape[2]
    block = rows // n
    split = [jnp.broadcast_to(p, (rows, LANES)) for p in pieces(squares)]
    split.append(jnp.zeros((rows, LANES), F32))
    outs = (own_ref, *sent)
    for i in range(4):
        total = None
        for j in range(2):
            copies[2 * i + j].wait()
            part = slice(j * half, (j + 1) * half)
            term = jnp.dot(normed[:, part], held[i, part], preferred_element_type=F32)
            total = term if total is None else total + term
        for s, out in enumerate(outs):
            here = slice(i * block, (i + 1) * block)
            out[here, :width] = total[s * block : (s + 1) * block].astype(out.dtype)
            out[here, width:] = split[i][s * block : (s + 1) * block].astype(out.dtype)


def read_kernel(n, own_ref, *refs):
    got, (cos_ref, sin_ref, gamma_ref, state_ref, kept_ref, key_ref, value_ref) = refs[: n - 1], refs[n - 1 :]
    block, head_dev, size, _ = state_ref.shape
    width = head_dev * size
    total = own_ref[...]
    for g in got:
        total = total + g[...].astype(F32)
    sq = total[:, width : width + 1]
    total_sq = sq[:block] + sq[block : 2 * block] + sq[2 * block : 3 * block]
    scale = lax.rsqrt(total_sq / D + 1e-06)
    query, key, value, gate = (total[i * block : (i + 1) * block, :width] * scale for i in range(4))
    value_ref[...] = value
    cos, sin = cos_ref[...], sin_ref[...]
    gate = gate / (1.0 + jnp.exp(-gate))
    for h in range(head_dev):
        at = slice(h * size, (h + 1) * size)
        q, k = query[:, at], key[:, at]
        q = q * cos + pltpu.roll(q, size // 2, 1) * sin
        k = (k * cos + pltpu.roll(k, size // 2, 1) * sin) * size ** (-0.5)
        key_ref[:, at] = k
        columns = jnp.concatenate([q, k], axis=0).T
        reads = []
        for b in range(block):
            reads.append(jnp.sum(columns[:, b : b + 1] * state_ref[b, h], axis=0, keepdims=True))
        match = jnp.sum(q * k, axis=1, keepdims=True)
        read = gamma_ref[h : h + 1, :] * jnp.concatenate(reads, axis=0) + match * value[:, at]
        read = read * lax.rsqrt(jnp.mean(read * read, axis=1, keepdims=True) + 1e-06)
        kept_ref[:, at] = (read * gate[:, at]).astype(BF16)


def update_kernel(key_ref, value_ref, gamma_ref, after_ref, state_ref, new_hbm, new_ref, sems):
    del after_ref
    block, head_dev, size, _ = state_ref.shape
    copies = []
    for h in range(head_dev):
        at = slice(h * size, (h + 1) * size)
        k = key_ref[:, at]
        columns = jnp.concatenate([k, k], axis=0).T
        gamma = gamma_ref[h : h + 1, :]
        for b in range(block):
            new_ref[b, h] = gamma * state_ref[b, h] + columns[:, b : b + 1] * value_ref[b : b + 1, at]
            copies.append(pltpu.make_async_copy(new_ref.at[b, h], new_hbm.at[b, h], sems.at[b, h]))
            copies[-1].start()
    for copy in copies:
        copy.wait()


def out_kernel(n, *refs):
    parts, (w_ref, own_ref, sent_ref) = refs[:n], refs[n:]
    kept = jnp.concatenate([p[...].astype(F32) for p in parts], axis=0).astype(BF16)
    kept = reorder(n, kept).astype(BF16)
    terms = jnp.dot(kept, w_ref[...], preferred_element_type=F32)
    own_ref[...] = terms
    sent_ref[...] = terms.astype(BF16)


def up_kernel(n_tp, n, x_ref, gain_ref, w_ref, own_ref, *refs):
    got, (mixed_ref, normed_ref, split_ref, *sent) = refs[: n_tp - 1], refs[n_tp - 1 :]
    total = own_ref[...]
    for g in got:
        total = total + g[...].astype(F32)
    mixed = (x_ref[...].astype(F32) + total).astype(BF16)
    mixed_ref[...] = mixed
    middle = mixed.astype(F32)
    normed = (middle * gain_ref[...]).astype(BF16)
    normed_ref[...] = normed
    rows = middle.shape[0]
    high, mid, low = pieces(jnp.sum(middle * middle, axis=1, keepdims=True))
    lane = lax.broadcasted_iota(jnp.int32, (rows, LANES), 1)
    split = jnp.where(lane == 0, high, jnp.where(lane == 1, mid, jnp.where(lane == 2, low, 0.0)))
    split_ref[...] = split
    part = w_ref.shape[1] // n
    me = lax.axis_index("kv")
    for s in reversed(range(1, n)):
        at = pl.ds(pl.multiple_of((me ^ s) * part, part), part)
        out = sent[s - 1]
        out[:, :part] = jnp.dot(normed, w_ref[:, at], preferred_element_type=F32).astype(out.dtype)
        out[:, part:] = split.astype(out.dtype)


def up_own_kernel(n, normed_ref, w_ref, out_ref):
    part = w_ref.shape[1] // n
    at = pl.ds(pl.multiple_of(lax.axis_index("kv") * part, part), part)
    out_ref[...] = jnp.dot(normed_ref[...], w_ref[:, at], preferred_element_type=F32)


def hidden_kernel(own_ref, split_ref, *refs):
    *got, out_ref = refs
    part = out_ref.shape[1]
    total, split = own_ref[...], split_ref[...]
    for g in got:
        total = total + g[:, :part].astype(F32)
        split = split + g[:, part:].astype(F32)
    sq = split[:, 0:1] + split[:, 1:2] + split[:, 2:3]
    scale = lax.rsqrt(sq / D + 1e-06)
    out_ref[...] = jnp.square(jnp.maximum(total * scale, 0.0)).astype(BF16)


def down_kernel(n, s, last, *refs):
    part_ref, w_ref, *refs = refs
    part = w_ref.shape[0] // n
    at = pl.ds(pl.multiple_of((lax.axis_index("kv") ^ s) * part, part), part)
    total = jnp.dot(part_ref[...], w_ref[at, :], preferred_element_type=F32)
    if s:
        total = total + refs.pop(0)[...]
    refs[0][...] = total
    if last:
        refs[1][...] = total.astype(BF16)


def final_kernel(mixed_ref, own_ref, *refs):
    *got, out_ref = refs
    total = own_ref[...]
    for g in got:
        total = total + g[...].astype(F32)
    out_ref[...] = (mixed_ref[...].astype(F32) + total).astype(BF16)


VMEM = pl.BlockSpec(memory_space=pltpu.VMEM)
HBM = pl.BlockSpec(memory_space=pltpu.HBM)


def call(kernel, name, outs, *args, specs=None, out_specs=None, scratch=(), limit=8, us=1):
    return pl.pallas_call(
        kernel,
        name=name,
        out_shape=[jax.ShapeDtypeStruct(*o) for o in outs],
        in_specs=specs or [VMEM] * len(args),
        out_specs=out_specs or [VMEM] * len(outs),
        scratch_shapes=scratch,
        compiler_params=pltpu.CompilerParams(vmem_limit_bytes=limit << 20),
        cost_estimate=pl.CostEstimate(flops=int(us * RATE), bytes_accessed=0, transcendentals=0),
    )(*args)


def far(value):
    return pltpu.with_memory_space_constraint(value, pltpu.HBM)


def near(value):
    return pltpu.with_memory_space_constraint(value, pltpu.VMEM)


def make_direct(n, n_tp):
    def shards(
        tokens, positions, state, norm_gain, w_query, w_key, w_value, w_gate, w_out, mlp_gain, w_up, w_down
    ):
        block, head_dev, size, _ = state.shape
        rows, depth = tokens.shape
        width = head_dev * size
        wide = width + LANES
        own, *sent = call(
            functools.partial(project_kernel, n),
            "project",
            [((4 * block, wide), F32)] + [((4 * block, wide), BF16)] * (n - 1),
            far(tokens),
            far(norm_gain[None]),
            far(w_query),
            far(w_key),
            far(w_value),
            far(w_gate),
            specs=[HBM] * 6,
            scratch=[
                pltpu.VMEM((rows, depth), BF16),
                pltpu.VMEM((1, depth), F32),
                pltpu.VMEM((4, depth, width), BF16),
                pltpu.SemaphoreType.DMA((4, 2)),
                pltpu.SemaphoreType.DMA((2,)),
            ],
            us=2,
        )
        got = [swap(sent[s - 1], "kv", n, s) for s in reversed(range(1, n))]
        half = size // 2
        freq = 10000.0 ** (-(jnp.arange(half, dtype=F32) * 2.0) / size)
        angle = positions.astype(F32)[:, None] * freq[None, :]
        cosine, sine = jnp.cos(angle), jnp.sin(angle)
        cosine = jnp.concatenate([cosine, cosine], axis=1)
        sine = jnp.concatenate([-sine, sine], axis=1)
        heads = (lax.axis_index("tp") * head_dev + jnp.arange(head_dev)).astype(F32)
        gamma = 1.0 - 2.0 ** (-5.0 - 5.0 * heads / (HEADS - 1))
        gamma = jnp.broadcast_to(gamma[:, None], (head_dev, size))
        state = near(state)
        kept, key, value = call(
            functools.partial(read_kernel, n),
            "read",
            [((block, width), BF16), ((block, width), F32), ((block, width), F32)],
            own,
            *got,
            cosine,
            sine,
            gamma,
            state,
            us=1,
        )
        kept = [kept] + [swap(kept, "kv", n, s) for s in range(1, n)]
        own, sent = call(
            functools.partial(out_kernel, n),
            "out",
            [((rows, depth), F32), ((rows, depth), BF16)],
            *kept,
            near(w_out),
        )
        got = [swap(sent, "tp", n_tp, s) for s in range(1, n_tp)]
        part = w_up.shape[1] // n
        w_up = near(w_up)
        mixed, normed, split, *sent = call(
            functools.partial(up_kernel, n_tp, n),
            "up",
            [((rows, depth), BF16), ((rows, depth), BF16), ((rows, LANES), F32)]
            + [((rows, part + LANES), BF16)] * (n - 1),
            tokens,
            mlp_gain[None],
            w_up,
            own,
            *got,
        )
        got = [swap(sent[s - 1], "kv", n, s) for s in reversed(range(1, n))]
        (new_state,) = call(
            update_kernel,
            "update",
            [(state.shape, F32)],
            key,
            value,
            gamma,
            split,
            state,
            out_specs=[HBM],
            scratch=[pltpu.VMEM(state.shape, F32), pltpu.SemaphoreType.DMA((block, head_dev))],
        )
        (own,) = call(
            functools.partial(up_own_kernel, n), "up_own", [((rows, part), F32)], normed, w_up
        )
        (hidden,) = call(hidden_kernel, "hidden", [((rows, part), BF16)], own, split, *got)
        got = [swap(hidden, "kv", n, s) for s in range(1, n)]
        w_down = near(w_down)
        (own,) = call(
            functools.partial(down_kernel, n, 0, False), "down_own", [((rows, depth), F32)], hidden, w_down
        )
        for s in reversed(range(1, n)):
            last = s == 1
            own, *sent = call(
                functools.partial(down_kernel, n, s, last),
                f"down_{s}",
                [((rows, depth), F32)] + [((rows, depth), BF16)] * last,
                got[s - 1],
                w_down,
                own,
            )
        (sent,) = sent
        got = [swap(sent, "tp", n_tp, s) for s in range(1, n_tp)]
        (layer_out,) = call(final_kernel, "final", [((rows, depth), BF16)], mixed, own, *got)
        return (layer_out, new_state)

    return shards


def solution(mesh):
    n_kv, n_tp = mesh.shape["kv"], mesh.shape["tp"]
    direct = all(n <= DIRECT and n & (n - 1) == 0 for n in (n_kv, n_tp))
    return jax.shard_map(
        make_direct(n_kv, n_tp) if direct else shards_large,
        mesh=mesh,
        in_specs=(
            P("grp", "kv"),
            P(("grp", "kv")),
            P(("grp", "kv"), "tp", None, None),
            P("kv"),
            P("kv", "tp"),
            P("kv", "tp"),
            P("kv", "tp"),
            P("kv", "tp"),
            P("tp", "kv"),
            P("kv"),
            P("kv", "tp"),
            P("tp", "kv"),
        ),
        out_specs=(P("grp", "kv"), P(("grp", "kv"), "tp", None, None)),
        check_vma=False,
    )
```

```python
import functools

import jax
import jax.numpy as jnp
from jax import lax
from jax.experimental import pallas as pl
from jax.experimental.pallas import tpu as pltpu
from jax.sharding import PartitionSpec as P

D = 4096
HEADS = 16
DIRECT = 8
LANES = 128
RATE = 1 << 33
F32, BF16 = jnp.float32, jnp.bfloat16


def turn(values, positions):
    half = values.shape[-1] // 2
    freq = 10000.0 ** (-(jnp.arange(half, dtype=jnp.float32) * 2.0) / values.shape[-1])
    angle = positions.astype(jnp.float32)[:, None, None] * freq[None, None, :]
    cosine = jnp.cos(angle)
    sine = jnp.sin(angle)
    first = values[..., :half]
    second = values[..., half:]
    return jnp.concatenate(
        [first * cosine - second * sine, first * sine + second * cosine], axis=-1
    )


def shards_large(
    tokens,
    positions,
    state,
    norm_gain,
    w_query,
    w_key,
    w_value,
    w_gate,
    w_out,
    mlp_gain,
    w_up,
    w_down,
):
    local_seqs, head_dev, head_size, _ = state.shape
    inputs = tokens.astype(jnp.float32)
    squares = jnp.sum(inputs * inputs, axis=1)
    normed = (inputs * norm_gain).astype(jnp.bfloat16)
    terms = jnp.stack(
        [
            jnp.dot(normed, weight, preferred_element_type=jnp.float32)
            for weight in (w_query, w_key, w_value, w_gate)
        ],
        axis=1,
    )
    summed, total_sq = (
        lax.psum_scatter(terms, "kv", scatter_dimension=0, tiled=True),
        lax.psum_scatter(squares, "kv", scatter_dimension=0, tiled=True),
    )
    scale1 = lax.rsqrt(total_sq / D + 1e-06)
    summed = (summed * scale1[:, None, None]).reshape(local_seqs, 4, head_dev, head_size)
    query = turn(summed[:, 0], positions)
    key_rows = turn(summed[:, 1], positions) * head_size ** (-0.5)
    value = summed[:, 2]
    gate = summed[:, 3]
    heads = (lax.axis_index("tp") * head_dev + jnp.arange(head_dev)).astype(jnp.float32)
    gamma = 1.0 - 2.0 ** (-5.0 - 5.0 * heads / (HEADS - 1))
    new_state = gamma[None, :, None, None] * state + key_rows[:, :, :, None] * value[:, :, None, :]
    read = jnp.einsum("bhd,bhde->bhe", query, new_state, precision=lax.Precision.HIGHEST)
    read = read * lax.rsqrt(jnp.mean(read * read, axis=-1, keepdims=True) + 1e-06)
    retained = (
        (read * jax.nn.silu(gate)).reshape(local_seqs, head_dev * head_size).astype(jnp.bfloat16)
    )
    head_terms = jnp.dot(
        lax.all_gather(retained, "kv", axis=0, tiled=True),
        w_out,
        preferred_element_type=jnp.float32,
    )
    mixed = (inputs + lax.psum(head_terms, "tp")).astype(jnp.bfloat16)
    middle = mixed.astype(jnp.float32)
    squares2 = jnp.sum(middle * middle, axis=1)
    normed2 = (middle * mlp_gain).astype(jnp.bfloat16)
    upward = jnp.dot(normed2, w_up, preferred_element_type=jnp.float32)
    up_full, total_sq2 = lax.psum((upward, squares2), "kv")
    scale2 = lax.rsqrt(total_sq2 / D + 1e-06)
    hidden = jnp.square(jax.nn.relu(up_full * scale2[:, None])).astype(jnp.bfloat16)
    down_terms = jnp.dot(hidden, w_down, preferred_element_type=jnp.float32)
    layer_out = (middle + lax.psum(down_terms, "tp")).astype(jnp.bfloat16)
    return (layer_out, new_state)


def swap(value, axis, n, step):
    return lax.ppermute(value, axis, [(i, i ^ step) for i in range(n)])


def pieces(value):
    high = value.astype(BF16).astype(F32)
    rest = value - high
    middle = rest.astype(BF16).astype(F32)
    return high, middle, rest - middle


def reorder(n, values):
    me = lax.axis_index("kv")
    rows = values.shape[0]
    block = rows // n
    to = lax.broadcasted_iota(jnp.int32, (rows, rows), 0)
    of = lax.broadcasted_iota(jnp.int32, (rows, rows), 1)
    hot = ((to // block) ^ me) * block + to % block == of
    return jnp.dot(hot.astype(F32).astype(BF16), values, preferred_element_type=F32)


def project_kernel(n, x_hbm, gain_hbm, *refs):
    weights, (own_ref, *sent), (x_ref, gain_ref, held, sems, small) = refs[:4], refs[4 : 4 + n], refs[4 + n :]
    first = [
        pltpu.make_async_copy(x_hbm, x_ref, small.at[0]),
        pltpu.make_async_copy(gain_hbm, gain_ref, small.at[1]),
    ]
    depth = x_ref.shape[1]
    half = depth // 2
    copies = []
    for i, w in enumerate(weights):
        for j in range(2):
            part = pl.ds(j * half, half)
            copies.append(pltpu.make_async_copy(w.at[part], held.at[i, part], sems.at[i, j]))
    for copy in first + copies:
        copy.start()
    first[0].wait()
    x = reorder(n, x_ref[...])
    squares = jnp.sum(x * x, axis=1, keepdims=True)
    first[1].wait()
    normed = (x * gain_ref[...]).astype(BF16)
    rows, width = x.shape[0], held.shape[2]
    block = rows // n
    split = [jnp.broadcast_to(p, (rows, LANES)) for p in pieces(squares)]
    split.append(jnp.zeros((rows, LANES), F32))
    outs = (own_ref, *sent)
    for i in range(4):
        total = None
        for j in range(2):
            copies[2 * i + j].wait()
            part = slice(j * half, (j + 1) * half)
            term = jnp.dot(normed[:, part], held[i, part], preferred_element_type=F32)
            total = term if total is None else total + term
        for s, out in enumerate(outs):
            here = slice(i * block, (i + 1) * block)
            out[here, :width] = total[s * block : (s + 1) * block].astype(out.dtype)
            out[here, width:] = split[i][s * block : (s + 1) * block].astype(out.dtype)


def read_kernel(n, own_ref, *refs):
    got, (cos_ref, sin_ref, gamma_ref, state_ref, kept_ref, key_ref, value_ref) = refs[: n - 1], refs[n - 1 :]
    block, head_dev, size, _ = state_ref.shape
    width = head_dev * size
    total = own_ref[...]
    for g in got:
        total = total + g[...].astype(F32)
    sq = total[:, width : width + 1]
    total_sq = sq[:block] + sq[block : 2 * block] + sq[2 * block : 3 * block]
    scale = lax.rsqrt(total_sq / D + 1e-06)
    query, key, value, gate = (total[i * block : (i + 1) * block, :width] * scale for i in range(4))
    value_ref[...] = value
    cos, sin = cos_ref[...], sin_ref[...]
    gate = gate / (1.0 + jnp.exp(-gate))
    for h in range(head_dev):
        at = slice(h * size, (h + 1) * size)
        q, k = query[:, at], key[:, at]
        q = q * cos + pltpu.roll(q, size // 2, 1) * sin
        k = (k * cos + pltpu.roll(k, size // 2, 1) * sin) * size ** (-0.5)
        key_ref[:, at] = k
        columns = jnp.concatenate([q, k], axis=0).T
        reads = []
        for b in range(block):
            reads.append(jnp.sum(columns[:, b : b + 1] * state_ref[b, h], axis=0, keepdims=True))
        match = jnp.sum(q * k, axis=1, keepdims=True)
        read = gamma_ref[h : h + 1, :] * jnp.concatenate(reads, axis=0) + match * value[:, at]
        read = read * lax.rsqrt(jnp.mean(read * read, axis=1, keepdims=True) + 1e-06)
        kept_ref[:, at] = (read * gate[:, at]).astype(BF16)


def update_kernel(key_ref, value_ref, gamma_ref, after_ref, state_ref, new_hbm, new_ref, sems):
    del after_ref
    block, head_dev, size, _ = state_ref.shape
    copies = []
    for h in range(head_dev):
        at = slice(h * size, (h + 1) * size)
        k = key_ref[:, at]
        columns = jnp.concatenate([k, k], axis=0).T
        gamma = gamma_ref[h : h + 1, :]
        for b in range(block):
            new_ref[b, h] = gamma * state_ref[b, h] + columns[:, b : b + 1] * value_ref[b : b + 1, at]
            copies.append(pltpu.make_async_copy(new_ref.at[b, h], new_hbm.at[b, h], sems.at[b, h]))
            copies[-1].start()
    for copy in copies:
        copy.wait()


def out_kernel(n, *refs):
    parts, (w_ref, own_ref, sent_ref) = refs[:n], refs[n:]
    kept = jnp.concatenate([p[...].astype(F32) for p in parts], axis=0).astype(BF16)
    kept = reorder(n, kept).astype(BF16)
    terms = jnp.dot(kept, w_ref[...], preferred_element_type=F32)
    own_ref[...] = terms
    sent_ref[...] = terms.astype(BF16)


def up_kernel(n_tp, n, x_ref, gain_ref, w_ref, own_ref, *refs):
    got, (mixed_ref, normed_ref, split_ref, *sent) = refs[: n_tp - 1], refs[n_tp - 1 :]
    total = own_ref[...]
    for g in got:
        total = total + g[...].astype(F32)
    mixed = (x_ref[...].astype(F32) + total).astype(BF16)
    mixed_ref[...] = mixed
    middle = mixed.astype(F32)
    normed = (middle * gain_ref[...]).astype(BF16)
    normed_ref[...] = normed
    rows = middle.shape[0]
    high, mid, low = pieces(jnp.sum(middle * middle, axis=1, keepdims=True))
    lane = lax.broadcasted_iota(jnp.int32, (rows, LANES), 1)
    split = jnp.where(lane == 0, high, jnp.where(lane == 1, mid, jnp.where(lane == 2, low, 0.0)))
    split_ref[...] = split
    part = w_ref.shape[1] // n
    me = lax.axis_index("kv")
    for s in reversed(range(1, n)):
        at = pl.ds(pl.multiple_of((me ^ s) * part, part), part)
        out = sent[s - 1]
        out[:, :part] = jnp.dot(normed, w_ref[:, at], preferred_element_type=F32).astype(out.dtype)
        out[:, part:] = split.astype(out.dtype)


def up_own_kernel(n, normed_ref, w_ref, out_ref):
    part = w_ref.shape[1] // n
    at = pl.ds(pl.multiple_of(lax.axis_index("kv") * part, part), part)
    out_ref[...] = jnp.dot(normed_ref[...], w_ref[:, at], preferred_element_type=F32)


def hidden_kernel(own_ref, split_ref, *refs):
    *got, out_ref = refs
    part = out_ref.shape[1]
    total, split = own_ref[...], split_ref[...]
    for g in got:
        total = total + g[:, :part].astype(F32)
        split = split + g[:, part:].astype(F32)
    sq = split[:, 0:1] + split[:, 1:2] + split[:, 2:3]
    scale = lax.rsqrt(sq / D + 1e-06)
    out_ref[...] = jnp.square(jnp.maximum(total * scale, 0.0)).astype(BF16)


def down_kernel(n, s, last, *refs):
    part_ref, w_ref, *refs = refs
    part = w_ref.shape[0] // n
    at = pl.ds(pl.multiple_of((lax.axis_index("kv") ^ s) * part, part), part)
    total = jnp.dot(part_ref[...], w_ref[at, :], preferred_element_type=F32)
    if s:
        total = total + refs.pop(0)[...]
    refs[0][...] = total
    if last:
        refs[1][...] = total.astype(BF16)


def final_kernel(mixed_ref, own_ref, *refs):
    *got, out_ref = refs
    total = own_ref[...]
    for g in got:
        total = total + g[...].astype(F32)
    out_ref[...] = (mixed_ref[...].astype(F32) + total).astype(BF16)


VMEM = pl.BlockSpec(memory_space=pltpu.VMEM)
HBM = pl.BlockSpec(memory_space=pltpu.HBM)


def call(kernel, name, outs, *args, specs=None, out_specs=None, scratch=(), limit=8, us=1, kept=True):
    return pl.pallas_call(
        kernel,
        name=name,
        out_shape=[(pltpu.VMEM if kept else jax.ShapeDtypeStruct)(*o) for o in outs],
        in_specs=specs or [VMEM] * len(args),
        out_specs=out_specs or [VMEM] * len(outs),
        scratch_shapes=scratch,
        compiler_params=pltpu.CompilerParams(vmem_limit_bytes=limit << 20),
        cost_estimate=pl.CostEstimate(flops=int(us * RATE), bytes_accessed=0, transcendentals=0),
    )(*args)


def far(value):
    return pltpu.with_memory_space_constraint(value, pltpu.HBM)


def near(value):
    return pltpu.with_memory_space_constraint(value, pltpu.VMEM)


def make_direct(n, n_tp):
    def shards(
        tokens, positions, state, norm_gain, w_query, w_key, w_value, w_gate, w_out, mlp_gain, w_up, w_down
    ):
        block, head_dev, size, _ = state.shape
        rows, depth = tokens.shape
        width = head_dev * size
        wide = width + LANES
        own, *sent = call(
            functools.partial(project_kernel, n),
            "project",
            [((4 * block, wide), F32)] + [((4 * block, wide), BF16)] * (n - 1),
            far(tokens),
            far(norm_gain[None]),
            far(w_query),
            far(w_key),
            far(w_value),
            far(w_gate),
            specs=[HBM] * 6,
            scratch=[
                pltpu.VMEM((rows, depth), BF16),
                pltpu.VMEM((1, depth), F32),
                pltpu.VMEM((4, depth, width), BF16),
                pltpu.SemaphoreType.DMA((4, 2)),
                pltpu.SemaphoreType.DMA((2,)),
            ],
            us=2,
        )
        got = [swap(sent[s - 1], "kv", n, s) for s in reversed(range(1, n))]
        half = size // 2
        freq = 10000.0 ** (-(jnp.arange(half, dtype=F32) * 2.0) / size)
        angle = positions.astype(F32)[:, None] * freq[None, :]
        cosine, sine = jnp.cos(angle), jnp.sin(angle)
        cosine = jnp.concatenate([cosine, cosine], axis=1)
        sine = jnp.concatenate([-sine, sine], axis=1)
        heads = (lax.axis_index("tp") * head_dev + jnp.arange(head_dev)).astype(F32)
        gamma = 1.0 - 2.0 ** (-5.0 - 5.0 * heads / (HEADS - 1))
        gamma = jnp.broadcast_to(gamma[:, None], (head_dev, size))
        state = near(state)
        kept, key, value = call(
            functools.partial(read_kernel, n),
            "read",
            [((block, width), BF16), ((block, width), F32), ((block, width), F32)],
            own,
            *got,
            cosine,
            sine,
            gamma,
            state,
            us=1,
        )
        kept = [kept] + [swap(kept, "kv", n, s) for s in range(1, n)]
        own, sent = call(
            functools.partial(out_kernel, n),
            "out",
            [((rows, depth), F32), ((rows, depth), BF16)],
            *kept,
            near(w_out),
        )
        got = [swap(sent, "tp", n_tp, s) for s in range(1, n_tp)]
        part = w_up.shape[1] // n
        w_up = near(w_up)
        mixed, normed, split, *sent = call(
            functools.partial(up_kernel, n_tp, n),
            "up",
            [((rows, depth), BF16), ((rows, depth), BF16), ((rows, LANES), F32)]
            + [((rows, part + LANES), BF16)] * (n - 1),
            tokens,
            mlp_gain[None],
            w_up,
            own,
            *got,
        )
        got = [swap(sent[s - 1], "kv", n, s) for s in reversed(range(1, n))]
        (new_state,) = call(
            update_kernel,
            "update",
            [(state.shape, F32)],
            key,
            value,
            gamma,
            split,
            state,
            out_specs=[HBM],
            scratch=[pltpu.VMEM(state.shape, F32), pltpu.SemaphoreType.DMA((block, head_dev))],
            kept=False,
        )
        (own,) = call(
            functools.partial(up_own_kernel, n), "up_own", [((rows, part), F32)], normed, w_up
        )
        (hidden,) = call(hidden_kernel, "hidden", [((rows, part), BF16)], own, split, *got)
        got = [swap(hidden, "kv", n, s) for s in range(1, n)]
        w_down = near(w_down)
        (own,) = call(
            functools.partial(down_kernel, n, 0, False), "down_own", [((rows, depth), F32)], hidden, w_down
        )
        for s in reversed(range(1, n)):
            last = s == 1
            own, *sent = call(
                functools.partial(down_kernel, n, s, last),
                f"down_{s}",
                [((rows, depth), F32)] + [((rows, depth), BF16)] * last,
                got[s - 1],
                w_down,
                own,
            )
        (sent,) = sent
        got = [swap(sent, "tp", n_tp, s) for s in range(1, n_tp)]
        (layer_out,) = call(final_kernel, "final", [((rows, depth), BF16)], mixed, own, *got, kept=False)
        return (layer_out, new_state)

    return shards


def solution(mesh):
    n_kv, n_tp = mesh.shape["kv"], mesh.shape["tp"]
    direct = all(n <= DIRECT and n & (n - 1) == 0 for n in (n_kv, n_tp))
    return jax.shard_map(
        make_direct(n_kv, n_tp) if direct else shards_large,
        mesh=mesh,
        in_specs=(
            P("grp", "kv"),
            P(("grp", "kv")),
            P(("grp", "kv"), "tp", None, None),
            P("kv"),
            P("kv", "tp"),
            P("kv", "tp"),
            P("kv", "tp"),
            P("kv", "tp"),
            P("tp", "kv"),
            P("kv"),
            P("kv", "tp"),
            P("tp", "kv"),
        ),
        out_specs=(P("grp", "kv"), P(("grp", "kv"), "tp", None, None)),
        check_vma=False,
    )
```

```python
import functools

import jax
import jax.numpy as jnp
from jax import lax
from jax.experimental import pallas as pl
from jax.experimental.pallas import tpu as pltpu
from jax.sharding import PartitionSpec as P

D = 4096
HEADS = 16
DIRECT = 8
LANES = 128
RATE = 1 << 33
F32, BF16 = jnp.float32, jnp.bfloat16


def turn(values, positions):
    half = values.shape[-1] // 2
    freq = 10000.0 ** (-(jnp.arange(half, dtype=jnp.float32) * 2.0) / values.shape[-1])
    angle = positions.astype(jnp.float32)[:, None, None] * freq[None, None, :]
    cosine = jnp.cos(angle)
    sine = jnp.sin(angle)
    first = values[..., :half]
    second = values[..., half:]
    return jnp.concatenate(
        [first * cosine - second * sine, first * sine + second * cosine], axis=-1
    )


def shards_large(
    tokens,
    positions,
    state,
    norm_gain,
    w_query,
    w_key,
    w_value,
    w_gate,
    w_out,
    mlp_gain,
    w_up,
    w_down,
):
    local_seqs, head_dev, head_size, _ = state.shape
    inputs = tokens.astype(jnp.float32)
    squares = jnp.sum(inputs * inputs, axis=1)
    normed = (inputs * norm_gain).astype(jnp.bfloat16)
    terms = jnp.stack(
        [
            jnp.dot(normed, weight, preferred_element_type=jnp.float32)
            for weight in (w_query, w_key, w_value, w_gate)
        ],
        axis=1,
    )
    summed, total_sq = (
        lax.psum_scatter(terms, "kv", scatter_dimension=0, tiled=True),
        lax.psum_scatter(squares, "kv", scatter_dimension=0, tiled=True),
    )
    scale1 = lax.rsqrt(total_sq / D + 1e-06)
    summed = (summed * scale1[:, None, None]).reshape(local_seqs, 4, head_dev, head_size)
    query = turn(summed[:, 0], positions)
    key_rows = turn(summed[:, 1], positions) * head_size ** (-0.5)
    value = summed[:, 2]
    gate = summed[:, 3]
    heads = (lax.axis_index("tp") * head_dev + jnp.arange(head_dev)).astype(jnp.float32)
    gamma = 1.0 - 2.0 ** (-5.0 - 5.0 * heads / (HEADS - 1))
    new_state = gamma[None, :, None, None] * state + key_rows[:, :, :, None] * value[:, :, None, :]
    read = jnp.einsum("bhd,bhde->bhe", query, new_state, precision=lax.Precision.HIGHEST)
    read = read * lax.rsqrt(jnp.mean(read * read, axis=-1, keepdims=True) + 1e-06)
    retained = (
        (read * jax.nn.silu(gate)).reshape(local_seqs, head_dev * head_size).astype(jnp.bfloat16)
    )
    head_terms = jnp.dot(
        lax.all_gather(retained, "kv", axis=0, tiled=True),
        w_out,
        preferred_element_type=jnp.float32,
    )
    mixed = (inputs + lax.psum(head_terms, "tp")).astype(jnp.bfloat16)
    middle = mixed.astype(jnp.float32)
    squares2 = jnp.sum(middle * middle, axis=1)
    normed2 = (middle * mlp_gain).astype(jnp.bfloat16)
    upward = jnp.dot(normed2, w_up, preferred_element_type=jnp.float32)
    up_full, total_sq2 = lax.psum((upward, squares2), "kv")
    scale2 = lax.rsqrt(total_sq2 / D + 1e-06)
    hidden = jnp.square(jax.nn.relu(up_full * scale2[:, None])).astype(jnp.bfloat16)
    down_terms = jnp.dot(hidden, w_down, preferred_element_type=jnp.float32)
    layer_out = (middle + lax.psum(down_terms, "tp")).astype(jnp.bfloat16)
    return (layer_out, new_state)


def swap(value, axis, n, step):
    return lax.ppermute(value, axis, [(i, i ^ step) for i in range(n)])


def pieces(value):
    high = value.astype(BF16).astype(F32)
    rest = value - high
    middle = rest.astype(BF16).astype(F32)
    return high, middle, rest - middle


def reorder(n, values):
    me = lax.axis_index("kv")
    rows = values.shape[0]
    block = rows // n
    to = lax.broadcasted_iota(jnp.int32, (rows, rows), 0)
    of = lax.broadcasted_iota(jnp.int32, (rows, rows), 1)
    hot = ((to // block) ^ me) * block + to % block == of
    return jnp.dot(hot.astype(F32).astype(BF16), values, preferred_element_type=F32)


def project_kernel(n, chunks, flight, x_hbm, gain_hbm, *refs):
    weights, outs, (x_ref, gain_ref, held, sems, small) = refs[:4], refs[4 : 4 + n], refs[4 + n :]
    first = [
        pltpu.make_async_copy(x_hbm, x_ref, small.at[0]),
        pltpu.make_async_copy(gain_hbm, gain_ref, small.at[1]),
    ]
    rows, depth = x_ref.shape
    width = held.shape[2]
    block, heads = rows // n, width // LANES
    step = depth // chunks
    copies = []
    for i, w in enumerate(weights):
        for j in range(chunks):
            part = pl.ds(j * step, step)
            copies.append(pltpu.make_async_copy(w.at[part], held.at[i, part], sems.at[i, j]))
    for copy in first + copies[:flight]:
        copy.start()
    first[0].wait()
    x = reorder(n, x_ref[...])
    lane = lax.broadcasted_iota(jnp.int32, (rows, LANES), 1)
    high, mid, low = pieces(jnp.sum(x * x, axis=1, keepdims=True))
    split = jnp.where(lane == 0, high, jnp.where(lane == 1, mid, jnp.where(lane == 2, low, 0.0)))
    group = heads * block
    for s, out in enumerate(outs):
        mine = split[s * block : (s + 1) * block]
        out[4 * group :] = jnp.concatenate([mine] * heads, axis=0).astype(out.dtype)
    first[1].wait()
    normed = (x * gain_ref[...]).astype(BF16)
    for i in range(4):
        total = None
        for j in range(chunks):
            at = chunks * i + j
            copies[at].wait()
            if at + flight < len(copies):
                copies[at + flight].start()
            part = slice(j * step, (j + 1) * step)
            term = jnp.dot(normed[:, part], held[i, part], preferred_element_type=F32)
            total = term if total is None else total + term
        for s, out in enumerate(outs):
            mine = total[s * block : (s + 1) * block]
            mine = jnp.concatenate([mine[:, h * LANES : (h + 1) * LANES] for h in range(heads)], axis=0)
            out[i * group : (i + 1) * group] = mine.astype(out.dtype)


def prepare_kernel(state_ref, cos_ref, sin_ref, out_ref, cosine_ref, sine_ref, gamma_ref):
    block, head_dev, size, _ = state_ref.shape
    for h in range(head_dev):
        for b in range(block):
            value = state_ref[b, h]
            high = value.astype(BF16)
            at = slice(b * size, (b + 1) * size)
            out_ref[h, :size, at] = high
            out_ref[h, size:, at] = (value - high.astype(F32)).astype(BF16)
    cos, sin = cos_ref[...], sin_ref[...]
    cosine_ref[...] = jnp.concatenate([jnp.concatenate([cos, cos], axis=1)] * head_dev, axis=0)
    sine_ref[...] = jnp.concatenate([jnp.concatenate([-sin, sin], axis=1)] * head_dev, axis=0)
    row = lax.broadcasted_iota(jnp.int32, gamma_ref.shape, 0)
    head = lax.axis_index("tp") * head_dev + row // block
    gamma_ref[...] = 1.0 - jnp.exp2(-5.0 - 5.0 * head.astype(F32) / (HEADS - 1))


def read_kernel(n, block, own_ref, *refs):
    got, (cos_ref, sin_ref, gamma_ref, prep_ref, kept_ref, key_ref, value_ref) = refs[: n - 1], refs[n - 1 :]
    head_dev, _, wide = prep_ref.shape
    size = wide // block
    total = own_ref[...]
    for g in got:
        total = total + g[...].astype(F32)
    group = head_dev * block
    sq = total[4 * group :]
    scale = lax.rsqrt((sq[:, 0:1] + sq[:, 1:2] + sq[:, 2:3]) / D + 1e-06)
    query, key, value, gate = (total[i * group : (i + 1) * group] * scale for i in range(4))
    cos, sin = cos_ref[...], sin_ref[...]
    query = query * cos + pltpu.roll(query, size // 2, 1) * sin
    high = query.astype(BF16).astype(F32)
    low = query - high
    row = lax.broadcasted_iota(jnp.int32, (2 * block, size), 0)
    reads = []
    for h in range(head_dev):
        at = slice(h * block, (h + 1) * block)
        both = jnp.concatenate([high[at], low[at]], axis=0).astype(BF16)
        both = jnp.concatenate([both, both], axis=1)
        product = jnp.dot(both, prep_ref[h], preferred_element_type=F32)
        picked = jnp.zeros((2 * block, size), F32)
        for b in range(block):
            picked = jnp.where(row % block == b, product[:, b * size : (b + 1) * size], picked)
        reads.append(picked[:block] + picked[block:])
    key = (key * cos + pltpu.roll(key, size // 2, 1) * sin) * size ** (-0.5)
    key_ref[...] = key
    value_ref[...] = value
    match = jnp.sum(query * key, axis=1, keepdims=True)
    gate = gate / (1.0 + jnp.exp(-gate))
    read = gamma_ref[...] * jnp.concatenate(reads, axis=0) + match * value
    read = read * lax.rsqrt(jnp.mean(read * read, axis=1, keepdims=True) + 1e-06)
    kept_ref[...] = (read * gate).astype(BF16)


def update_kernel(key_ref, value_ref, gamma_ref, after_ref, state_ref, new_hbm, new_ref, sems):
    del after_ref
    block, head_dev, size, _ = state_ref.shape
    copies = []
    for h in range(head_dev):
        rows = slice(h * block, (h + 1) * block)
        k, v = key_ref[rows], value_ref[rows]
        columns = jnp.concatenate([k, k], axis=0).T
        gamma = gamma_ref[h * block : h * block + 1, :]
        for b in range(block):
            new_ref[b, h] = gamma * state_ref[b, h] + columns[:, b : b + 1] * v[b : b + 1]
            copies.append(pltpu.make_async_copy(new_ref.at[b, h], new_hbm.at[b, h], sems.at[b, h]))
            copies[-1].start()
    for copy in copies:
        copy.wait()


def out_kernel(n, *refs):
    parts, (w_ref, own_ref, sent_ref) = refs[:n], refs[n:]
    kept = jnp.concatenate([p[...] for p in parts], axis=0)
    many, size = kept.shape
    heads = w_ref.shape[0] // size
    block = many // n // heads
    rows = n * block
    me = lax.axis_index("kv")
    to = lax.broadcasted_iota(jnp.int32, (many, many), 0)
    of = lax.broadcasted_iota(jnp.int32, (many, many), 1)
    head, row = to // rows, to % rows
    hot = ((row // block) ^ me) * (heads * block) + head * block + row % block == of
    kept = jnp.dot(hot.astype(F32).astype(BF16), kept, preferred_element_type=F32).astype(BF16)
    kept = jnp.concatenate([kept[h * rows : (h + 1) * rows] for h in range(heads)], axis=1)
    terms = jnp.dot(kept, w_ref[...], preferred_element_type=F32)
    own_ref[...] = terms
    sent_ref[...] = terms.astype(BF16)


def up_kernel(n_tp, n, x_ref, gain_ref, w_ref, own_ref, *refs):
    got, (mixed_ref, normed_ref, split_ref, *sent) = refs[: n_tp - 1], refs[n_tp - 1 :]
    total = own_ref[...]
    for g in got:
        total = total + g[...].astype(F32)
    mixed = (x_ref[...].astype(F32) + total).astype(BF16)
    mixed_ref[...] = mixed
    middle = mixed.astype(F32)
    normed = (middle * gain_ref[...]).astype(BF16)
    normed_ref[...] = normed
    rows = middle.shape[0]
    high, mid, low = pieces(jnp.sum(middle * middle, axis=1, keepdims=True))
    lane = lax.broadcasted_iota(jnp.int32, (rows, LANES), 1)
    split = jnp.where(lane == 0, high, jnp.where(lane == 1, mid, jnp.where(lane == 2, low, 0.0)))
    split_ref[...] = split
    part = w_ref.shape[1] // n
    me = lax.axis_index("kv")
    for s in reversed(range(1, n)):
        at = pl.ds(pl.multiple_of((me ^ s) * part, part), part)
        out = sent[s - 1]
        out[:, :part] = jnp.dot(normed, w_ref[:, at], preferred_element_type=F32).astype(out.dtype)
        out[:, part:] = split.astype(out.dtype)


def up_own_kernel(n, normed_ref, w_ref, out_ref):
    part = w_ref.shape[1] // n
    at = pl.ds(pl.multiple_of(lax.axis_index("kv") * part, part), part)
    out_ref[...] = jnp.dot(normed_ref[...], w_ref[:, at], preferred_element_type=F32)


def hidden_kernel(own_ref, split_ref, *refs):
    *got, out_ref = refs
    part = out_ref.shape[1]
    total, split = own_ref[...], split_ref[...]
    for g in got:
        total = total + g[:, :part].astype(F32)
        split = split + g[:, part:].astype(F32)
    sq = split[:, 0:1] + split[:, 1:2] + split[:, 2:3]
    scale = lax.rsqrt(sq / D + 1e-06)
    out_ref[...] = jnp.square(jnp.maximum(total * scale, 0.0)).astype(BF16)


def down_kernel(n, s, last, *refs):
    part_ref, w_ref, *refs = refs
    part = w_ref.shape[0] // n
    at = pl.ds(pl.multiple_of((lax.axis_index("kv") ^ s) * part, part), part)
    total = jnp.dot(part_ref[...], w_ref[at, :], preferred_element_type=F32)
    if s:
        total = total + refs.pop(0)[...]
    refs[0][...] = total
    if last:
        refs[1][...] = total.astype(BF16)


def final_kernel(mixed_ref, own_ref, *refs):
    *got, out_ref = refs
    total = own_ref[...]
    for g in got:
        total = total + g[...].astype(F32)
    out_ref[...] = (mixed_ref[...].astype(F32) + total).astype(BF16)


VMEM = pl.BlockSpec(memory_space=pltpu.VMEM)
HBM = pl.BlockSpec(memory_space=pltpu.HBM)


def call(kernel, name, outs, *args, specs=None, out_specs=None, scratch=(), limit=8, us=1, kept=True):
    return pl.pallas_call(
        kernel,
        name=name,
        out_shape=[(pltpu.VMEM if kept else jax.ShapeDtypeStruct)(*o) for o in outs],
        in_specs=specs or [VMEM] * len(args),
        out_specs=out_specs or [VMEM] * len(outs),
        scratch_shapes=scratch,
        compiler_params=pltpu.CompilerParams(vmem_limit_bytes=limit << 20),
        cost_estimate=pl.CostEstimate(flops=int(us * RATE), bytes_accessed=0, transcendentals=0),
    )(*args)


def far(value):
    return pltpu.with_memory_space_constraint(value, pltpu.HBM)


def near(value):
    return pltpu.with_memory_space_constraint(value, pltpu.VMEM)


def make_direct(n, n_tp):
    def shards(
        tokens, positions, state, norm_gain, w_query, w_key, w_value, w_gate, w_out, mlp_gain, w_up, w_down
    ):
        block, head_dev, size, _ = state.shape
        rows, depth = tokens.shape
        width = head_dev * size
        group = head_dev * block
        chunks, flight = 1, 4
        own, *sent = call(
            functools.partial(project_kernel, n, chunks, flight),
            "project",
            [((5 * group, size), F32)] + [((5 * group, size), BF16)] * (n - 1),
            far(tokens),
            far(norm_gain[None]),
            far(w_query),
            far(w_key),
            far(w_value),
            far(w_gate),
            specs=[HBM] * 6,
            scratch=[
                pltpu.VMEM((rows, depth), BF16),
                pltpu.VMEM((1, depth), F32),
                pltpu.VMEM((4, depth, width), BF16),
                pltpu.SemaphoreType.DMA((4, chunks)),
                pltpu.SemaphoreType.DMA((2,)),
            ],
            us=2,
        )
        got = [swap(sent[s - 1], "kv", n, s) for s in reversed(range(1, n))]
        half = size // 2
        freq = 10000.0 ** (-(jnp.arange(half, dtype=F32) * 2.0) / size)
        angle = positions.astype(F32)[:, None] * freq[None, :]
        cosine, sine = jnp.cos(angle), jnp.sin(angle)
        state = near(state)
        prepared, cosine, sine, gamma = call(
            prepare_kernel,
            "prepare",
            [((head_dev, 2 * size, block * size), BF16)] + [((group, size), F32)] * 3,
            state,
            cosine,
            sine,
        )
        kept, key, value = call(
            functools.partial(read_kernel, n, block),
            "read",
            [((group, size), BF16), ((group, size), F32), ((group, size), F32)],
            own,
            *got,
            cosine,
            sine,
            gamma,
            prepared,
        )
        kept = [kept] + [swap(kept, "kv", n, s) for s in range(1, n)]
        own, sent = call(
            functools.partial(out_kernel, n),
            "out",
            [((rows, depth), F32), ((rows, depth), BF16)],
            *kept,
            near(w_out),
        )
        got = [swap(sent, "tp", n_tp, s) for s in range(1, n_tp)]
        part = w_up.shape[1] // n
        w_up = near(w_up)
        mixed, normed, split, *sent = call(
            functools.partial(up_kernel, n_tp, n),
            "up",
            [((rows, depth), BF16), ((rows, depth), BF16), ((rows, LANES), F32)]
            + [((rows, part + LANES), BF16)] * (n - 1),
            tokens,
            mlp_gain[None],
            w_up,
            own,
            *got,
        )
        got = [swap(sent[s - 1], "kv", n, s) for s in reversed(range(1, n))]
        (new_state,) = call(
            update_kernel,
            "update",
            [(state.shape, F32)],
            key,
            value,
            gamma,
            split,
            state,
            out_specs=[HBM],
            scratch=[pltpu.VMEM(state.shape, F32), pltpu.SemaphoreType.DMA((block, head_dev))],
            kept=False,
        )
        (own,) = call(
            functools.partial(up_own_kernel, n), "up_own", [((rows, part), F32)], normed, w_up
        )
        (hidden,) = call(hidden_kernel, "hidden", [((rows, part), BF16)], own, split, *got)
        got = [swap(hidden, "kv", n, s) for s in range(1, n)]
        w_down = near(w_down)
        (own,) = call(
            functools.partial(down_kernel, n, 0, False), "down_own", [((rows, depth), F32)], hidden, w_down
        )
        for s in reversed(range(1, n)):
            last = s == 1
            own, *sent = call(
                functools.partial(down_kernel, n, s, last),
                f"down_{s}",
                [((rows, depth), F32)] + [((rows, depth), BF16)] * last,
                got[s - 1],
                w_down,
                own,
            )
        (sent,) = sent
        got = [swap(sent, "tp", n_tp, s) for s in range(1, n_tp)]
        (layer_out,) = call(final_kernel, "final", [((rows, depth), BF16)], mixed, own, *got, kept=False)
        return (layer_out, new_state)

    return shards


def solution(mesh):
    n_kv, n_tp = mesh.shape["kv"], mesh.shape["tp"]
    direct = all(n <= DIRECT and n & (n - 1) == 0 for n in (n_kv, n_tp))
    return jax.shard_map(
        make_direct(n_kv, n_tp) if direct else shards_large,
        mesh=mesh,
        in_specs=(
            P("grp", "kv"),
            P(("grp", "kv")),
            P(("grp", "kv"), "tp", None, None),
            P("kv"),
            P("kv", "tp"),
            P("kv", "tp"),
            P("kv", "tp"),
            P("kv", "tp"),
            P("tp", "kv"),
            P("kv"),
            P("kv", "tp"),
            P("tp", "kv"),
        ),
        out_specs=(P("grp", "kv"), P(("grp", "kv"), "tp", None, None)),
        check_vma=False,
    )
```

```python
import functools

import jax
import jax.numpy as jnp
from jax import lax
from jax.experimental import pallas as pl
from jax.experimental.pallas import tpu as pltpu
from jax.sharding import PartitionSpec as P

D = 4096
HEADS = 16
DIRECT = 8
LANES = 128
ORDERS = ((2, 3, 1), (2, 3, 1), (3, 2, 1), (2, 3, 1), (2, 3, 1), (3, 2, 1))
RATE = 1 << 33
F32, BF16 = jnp.float32, jnp.bfloat16


def turn(values, positions):
    half = values.shape[-1] // 2
    freq = 10000.0 ** (-(jnp.arange(half, dtype=jnp.float32) * 2.0) / values.shape[-1])
    angle = positions.astype(jnp.float32)[:, None, None] * freq[None, None, :]
    cosine = jnp.cos(angle)
    sine = jnp.sin(angle)
    first = values[..., :half]
    second = values[..., half:]
    return jnp.concatenate(
        [first * cosine - second * sine, first * sine + second * cosine], axis=-1
    )


def shards_large(
    tokens,
    positions,
    state,
    norm_gain,
    w_query,
    w_key,
    w_value,
    w_gate,
    w_out,
    mlp_gain,
    w_up,
    w_down,
):
    local_seqs, head_dev, head_size, _ = state.shape
    inputs = tokens.astype(jnp.float32)
    squares = jnp.sum(inputs * inputs, axis=1)
    normed = (inputs * norm_gain).astype(jnp.bfloat16)
    terms = jnp.stack(
        [
            jnp.dot(normed, weight, preferred_element_type=jnp.float32)
            for weight in (w_query, w_key, w_value, w_gate)
        ],
        axis=1,
    )
    summed, total_sq = (
        lax.psum_scatter(terms, "kv", scatter_dimension=0, tiled=True),
        lax.psum_scatter(squares, "kv", scatter_dimension=0, tiled=True),
    )
    scale1 = lax.rsqrt(total_sq / D + 1e-06)
    summed = (summed * scale1[:, None, None]).reshape(local_seqs, 4, head_dev, head_size)
    query = turn(summed[:, 0], positions)
    key_rows = turn(summed[:, 1], positions) * head_size ** (-0.5)
    value = summed[:, 2]
    gate = summed[:, 3]
    heads = (lax.axis_index("tp") * head_dev + jnp.arange(head_dev)).astype(jnp.float32)
    gamma = 1.0 - 2.0 ** (-5.0 - 5.0 * heads / (HEADS - 1))
    new_state = gamma[None, :, None, None] * state + key_rows[:, :, :, None] * value[:, :, None, :]
    read = jnp.einsum("bhd,bhde->bhe", query, new_state, precision=lax.Precision.HIGHEST)
    read = read * lax.rsqrt(jnp.mean(read * read, axis=-1, keepdims=True) + 1e-06)
    retained = (
        (read * jax.nn.silu(gate)).reshape(local_seqs, head_dev * head_size).astype(jnp.bfloat16)
    )
    head_terms = jnp.dot(
        lax.all_gather(retained, "kv", axis=0, tiled=True),
        w_out,
        preferred_element_type=jnp.float32,
    )
    mixed = (inputs + lax.psum(head_terms, "tp")).astype(jnp.bfloat16)
    middle = mixed.astype(jnp.float32)
    squares2 = jnp.sum(middle * middle, axis=1)
    normed2 = (middle * mlp_gain).astype(jnp.bfloat16)
    upward = jnp.dot(normed2, w_up, preferred_element_type=jnp.float32)
    up_full, total_sq2 = lax.psum((upward, squares2), "kv")
    scale2 = lax.rsqrt(total_sq2 / D + 1e-06)
    hidden = jnp.square(jax.nn.relu(up_full * scale2[:, None])).astype(jnp.bfloat16)
    down_terms = jnp.dot(hidden, w_down, preferred_element_type=jnp.float32)
    layer_out = (middle + lax.psum(down_terms, "tp")).astype(jnp.bfloat16)
    return (layer_out, new_state)


def exchange(values, axis, n, order):
    steps = [s for s in order if s < n] + [s for s in reversed(range(1, n)) if s not in order]
    if not isinstance(values, list):
        steps, values = steps[::-1], [values] * (n - 1)
    return [swap(values[s - 1], axis, n, s) for s in steps], steps


def swap(value, axis, n, step):
    return lax.ppermute(value, axis, [(i, i ^ step) for i in range(n)])


def pieces(value):
    high = value.astype(BF16).astype(F32)
    rest = value - high
    middle = rest.astype(BF16).astype(F32)
    return high, middle, rest - middle


def reorder(n, values):
    me = lax.axis_index("kv")
    rows = values.shape[0]
    block = rows // n
    to = lax.broadcasted_iota(jnp.int32, (rows, rows), 0)
    of = lax.broadcasted_iota(jnp.int32, (rows, rows), 1)
    hot = ((to // block) ^ me) * block + to % block == of
    return jnp.dot(hot.astype(F32).astype(BF16), values, preferred_element_type=F32)


def project_kernel(n, chunks, flight, x_hbm, gain_hbm, *refs):
    weights, outs, (x_ref, gain_ref, held, sems, small) = refs[:4], refs[4 : 4 + n], refs[4 + n :]
    first = [
        pltpu.make_async_copy(x_hbm, x_ref, small.at[0]),
        pltpu.make_async_copy(gain_hbm, gain_ref, small.at[1]),
    ]
    rows, depth = x_ref.shape
    width = held.shape[2]
    block, heads = rows // n, width // LANES
    step = depth // chunks
    copies = []
    for i, w in enumerate(weights):
        for j in range(chunks):
            part = pl.ds(j * step, step)
            copies.append(pltpu.make_async_copy(w.at[part], held.at[i, part], sems.at[i, j]))
    for copy in first + copies[:flight]:
        copy.start()
    first[0].wait()
    x = reorder(n, x_ref[...])
    lane = lax.broadcasted_iota(jnp.int32, (rows, LANES), 1)
    high, mid, low = pieces(jnp.sum(x * x, axis=1, keepdims=True))
    split = jnp.where(lane == 0, high, jnp.where(lane == 1, mid, jnp.where(lane == 2, low, 0.0)))
    group = heads * block
    for s, out in enumerate(outs):
        mine = split[s * block : (s + 1) * block]
        out[4 * group :] = jnp.concatenate([mine] * heads, axis=0).astype(out.dtype)
    first[1].wait()
    normed = (x * gain_ref[...]).astype(BF16)
    for i in range(4):
        total = None
        for j in range(chunks):
            at = chunks * i + j
            copies[at].wait()
            if at + flight < len(copies):
                copies[at + flight].start()
            part = slice(j * step, (j + 1) * step)
            term = jnp.dot(normed[:, part], held[i, part], preferred_element_type=F32)
            total = term if total is None else total + term
        for s, out in enumerate(outs):
            mine = total[s * block : (s + 1) * block]
            mine = jnp.concatenate([mine[:, h * LANES : (h + 1) * LANES] for h in range(heads)], axis=0)
            out[i * group : (i + 1) * group] = mine.astype(out.dtype)


def prepare_kernel(state_ref, cos_ref, sin_ref, out_ref, cosine_ref, sine_ref, gamma_ref):
    block, head_dev, size, _ = state_ref.shape
    for h in range(head_dev):
        for b in range(block):
            value = state_ref[b, h]
            high = value.astype(BF16)
            at = slice(b * size, (b + 1) * size)
            out_ref[h, :size, at] = high
            out_ref[h, size:, at] = (value - high.astype(F32)).astype(BF16)
    cos, sin = cos_ref[...], sin_ref[...]
    cosine_ref[...] = jnp.concatenate([jnp.concatenate([cos, cos], axis=1)] * head_dev, axis=0)
    sine_ref[...] = jnp.concatenate([jnp.concatenate([-sin, sin], axis=1)] * head_dev, axis=0)
    row = lax.broadcasted_iota(jnp.int32, gamma_ref.shape, 0)
    head = lax.axis_index("tp") * head_dev + row // block
    gamma_ref[...] = 1.0 - jnp.exp2(-5.0 - 5.0 * head.astype(F32) / (HEADS - 1))


def read_kernel(n, block, own_ref, *refs):
    got, (cos_ref, sin_ref, gamma_ref, prep_ref, kept_ref, key_ref, value_ref) = refs[: n - 1], refs[n - 1 :]
    head_dev, _, wide = prep_ref.shape
    size = wide // block
    total = own_ref[...]
    for g in got:
        total = total + g[...].astype(F32)
    group = head_dev * block
    sq = total[4 * group :]
    scale = lax.rsqrt((sq[:, 0:1] + sq[:, 1:2] + sq[:, 2:3]) / D + 1e-06)
    query, key, value, gate = (total[i * group : (i + 1) * group] * scale for i in range(4))
    cos, sin = cos_ref[...], sin_ref[...]
    query = query * cos + pltpu.roll(query, size // 2, 1) * sin
    high = query.astype(BF16).astype(F32)
    low = query - high
    row = lax.broadcasted_iota(jnp.int32, (2 * block, size), 0)
    reads = []
    for h in range(head_dev):
        at = slice(h * block, (h + 1) * block)
        both = jnp.concatenate([high[at], low[at]], axis=0).astype(BF16)
        both = jnp.concatenate([both, both], axis=1)
        product = jnp.dot(both, prep_ref[h], preferred_element_type=F32)
        picked = jnp.zeros((2 * block, size), F32)
        for b in range(block):
            picked = jnp.where(row % block == b, product[:, b * size : (b + 1) * size], picked)
        reads.append(picked[:block] + picked[block:])
    key = (key * cos + pltpu.roll(key, size // 2, 1) * sin) * size ** (-0.5)
    key_ref[...] = key
    value_ref[...] = value
    match = jnp.sum(query * key, axis=1, keepdims=True)
    gate = gate / (1.0 + jnp.exp(-gate))
    read = gamma_ref[...] * jnp.concatenate(reads, axis=0) + match * value
    read = read * lax.rsqrt(jnp.mean(read * read, axis=1, keepdims=True) + 1e-06)
    kept_ref[...] = (read * gate).astype(BF16)


def update_kernel(key_ref, value_ref, gamma_ref, after_ref, state_ref, new_hbm, new_ref, sems):
    del after_ref
    block, head_dev, size, _ = state_ref.shape
    copies = []
    for h in range(head_dev):
        rows = slice(h * block, (h + 1) * block)
        k, v = key_ref[rows], value_ref[rows]
        columns = jnp.concatenate([k, k], axis=0).T
        gamma = gamma_ref[h * block : h * block + 1, :]
        for b in range(block):
            new_ref[b, h] = gamma * state_ref[b, h] + columns[:, b : b + 1] * v[b : b + 1]
            copies.append(pltpu.make_async_copy(new_ref.at[b, h], new_hbm.at[b, h], sems.at[b, h]))
            copies[-1].start()
    for copy in copies:
        copy.wait()


def out_kernel(steps, *refs):
    n = len(steps)
    parts, (w_ref, own_ref, sent_ref) = refs[:n], refs[n:]
    kept = jnp.concatenate([p[...] for p in parts], axis=0)
    many, size = kept.shape
    heads = w_ref.shape[0] // size
    block = many // n // heads
    rows = n * block
    me = lax.axis_index("kv")
    to = lax.broadcasted_iota(jnp.int32, (many, many), 0)
    of = lax.broadcasted_iota(jnp.int32, (many, many), 1)
    head, row = to // rows, to % rows
    part = of // (heads * block)
    owner = sum(jnp.where(part == i, me ^ s, 0) for i, s in enumerate(steps))
    hot = (owner == row // block) & (of % (heads * block) == head * block + row % block)
    kept = jnp.dot(hot.astype(F32).astype(BF16), kept, preferred_element_type=F32).astype(BF16)
    kept = jnp.concatenate([kept[h * rows : (h + 1) * rows] for h in range(heads)], axis=1)
    terms = jnp.dot(kept, w_ref[...], preferred_element_type=F32)
    own_ref[...] = terms
    sent_ref[...] = terms.astype(BF16)


def up_kernel(n_tp, n, x_ref, gain_ref, w_ref, own_ref, *refs):
    got, (mixed_ref, normed_ref, split_ref, *sent) = refs[: n_tp - 1], refs[n_tp - 1 :]
    total = own_ref[...]
    for g in got:
        total = total + g[...].astype(F32)
    mixed = (x_ref[...].astype(F32) + total).astype(BF16)
    mixed_ref[...] = mixed
    middle = mixed.astype(F32)
    normed = (middle * gain_ref[...]).astype(BF16)
    normed_ref[...] = normed
    rows = middle.shape[0]
    high, mid, low = pieces(jnp.sum(middle * middle, axis=1, keepdims=True))
    lane = lax.broadcasted_iota(jnp.int32, (rows, LANES), 1)
    split = jnp.where(lane == 0, high, jnp.where(lane == 1, mid, jnp.where(lane == 2, low, 0.0)))
    split_ref[...] = split
    part = w_ref.shape[1] // n
    me = lax.axis_index("kv")
    for s in reversed(range(1, n)):
        at = pl.ds(pl.multiple_of((me ^ s) * part, part), part)
        out = sent[s - 1]
        out[:, :part] = jnp.dot(normed, w_ref[:, at], preferred_element_type=F32).astype(out.dtype)
        out[:, part:] = split.astype(out.dtype)


def up_own_kernel(n, normed_ref, w_ref, out_ref):
    part = w_ref.shape[1] // n
    at = pl.ds(pl.multiple_of(lax.axis_index("kv") * part, part), part)
    out_ref[...] = jnp.dot(normed_ref[...], w_ref[:, at], preferred_element_type=F32)


def hidden_kernel(own_ref, split_ref, *refs):
    *got, out_ref = refs
    part = out_ref.shape[1]
    total, split = own_ref[...], split_ref[...]
    for g in got:
        total = total + g[:, :part].astype(F32)
        split = split + g[:, part:].astype(F32)
    sq = split[:, 0:1] + split[:, 1:2] + split[:, 2:3]
    scale = lax.rsqrt(sq / D + 1e-06)
    out_ref[...] = jnp.square(jnp.maximum(total * scale, 0.0)).astype(BF16)


def down_kernel(n, s, last, *refs):
    part_ref, w_ref, *refs = refs
    part = w_ref.shape[0] // n
    at = pl.ds(pl.multiple_of((lax.axis_index("kv") ^ s) * part, part), part)
    total = jnp.dot(part_ref[...], w_ref[at, :], preferred_element_type=F32)
    if s:
        total = total + refs.pop(0)[...]
    refs[0][...] = total
    if last:
        refs[1][...] = total.astype(BF16)


def final_kernel(mixed_ref, own_ref, *refs):
    *got, out_ref = refs
    total = own_ref[...]
    for g in got:
        total = total + g[...].astype(F32)
    out_ref[...] = (mixed_ref[...].astype(F32) + total).astype(BF16)


VMEM = pl.BlockSpec(memory_space=pltpu.VMEM)
HBM = pl.BlockSpec(memory_space=pltpu.HBM)


def call(kernel, name, outs, *args, specs=None, out_specs=None, scratch=(), limit=8, us=1, kept=True):
    return pl.pallas_call(
        kernel,
        name=name,
        out_shape=[(pltpu.VMEM if kept else jax.ShapeDtypeStruct)(*o) for o in outs],
        in_specs=specs or [VMEM] * len(args),
        out_specs=out_specs or [VMEM] * len(outs),
        scratch_shapes=scratch,
        compiler_params=pltpu.CompilerParams(vmem_limit_bytes=limit << 20),
        cost_estimate=pl.CostEstimate(flops=int(us * RATE), bytes_accessed=0, transcendentals=0),
    )(*args)


def far(value):
    return pltpu.with_memory_space_constraint(value, pltpu.HBM)


def near(value):
    return pltpu.with_memory_space_constraint(value, pltpu.VMEM)


def make_direct(n, n_tp):
    def shards(
        tokens, positions, state, norm_gain, w_query, w_key, w_value, w_gate, w_out, mlp_gain, w_up, w_down
    ):
        block, head_dev, size, _ = state.shape
        rows, depth = tokens.shape
        width = head_dev * size
        group = head_dev * block
        chunks, flight = 1, 4
        own, *sent = call(
            functools.partial(project_kernel, n, chunks, flight),
            "project",
            [((5 * group, size), F32)] + [((5 * group, size), BF16)] * (n - 1),
            far(tokens),
            far(norm_gain[None]),
            far(w_query),
            far(w_key),
            far(w_value),
            far(w_gate),
            specs=[HBM] * 6,
            scratch=[
                pltpu.VMEM((rows, depth), BF16),
                pltpu.VMEM((1, depth), F32),
                pltpu.VMEM((4, depth, width), BF16),
                pltpu.SemaphoreType.DMA((4, chunks)),
                pltpu.SemaphoreType.DMA((2,)),
            ],
            us=2,
        )
        got, _ = exchange(sent, "kv", n, ORDERS[0])
        half = size // 2
        freq = 10000.0 ** (-(jnp.arange(half, dtype=F32) * 2.0) / size)
        angle = positions.astype(F32)[:, None] * freq[None, :]
        cosine, sine = jnp.cos(angle), jnp.sin(angle)
        state = near(state)
        prepared, cosine, sine, gamma = call(
            prepare_kernel,
            "prepare",
            [((head_dev, 2 * size, block * size), BF16)] + [((group, size), F32)] * 3,
            state,
            cosine,
            sine,
        )
        kept, key, value = call(
            functools.partial(read_kernel, n, block),
            "read",
            [((group, size), BF16), ((group, size), F32), ((group, size), F32)],
            own,
            *got,
            cosine,
            sine,
            gamma,
            prepared,
        )
        got, steps = exchange(kept, "kv", n, ORDERS[1])
        own, sent = call(
            functools.partial(out_kernel, (0, *steps)),
            "out",
            [((rows, depth), F32), ((rows, depth), BF16)],
            kept,
            *got,
            near(w_out),
        )
        got, _ = exchange(sent, "tp", n_tp, ORDERS[2])
        part = w_up.shape[1] // n
        w_up = near(w_up)
        mixed, normed, split, *sent = call(
            functools.partial(up_kernel, n_tp, n),
            "up",
            [((rows, depth), BF16), ((rows, depth), BF16), ((rows, LANES), F32)]
            + [((rows, part + LANES), BF16)] * (n - 1),
            tokens,
            mlp_gain[None],
            w_up,
            own,
            *got,
        )
        got, _ = exchange(sent, "kv", n, ORDERS[3])
        (new_state,) = call(
            update_kernel,
            "update",
            [(state.shape, F32)],
            key,
            value,
            gamma,
            split,
            state,
            out_specs=[HBM],
            scratch=[pltpu.VMEM(state.shape, F32), pltpu.SemaphoreType.DMA((block, head_dev))],
            kept=False,
        )
        (own,) = call(
            functools.partial(up_own_kernel, n), "up_own", [((rows, part), F32)], normed, w_up
        )
        (hidden,) = call(hidden_kernel, "hidden", [((rows, part), BF16)], own, split, *got)
        got, steps = exchange(hidden, "kv", n, ORDERS[4])
        w_down = near(w_down)
        (own,) = call(
            functools.partial(down_kernel, n, 0, False), "down_own", [((rows, depth), F32)], hidden, w_down
        )
        for i, s in reversed(list(enumerate(steps))):
            last = i == 0
            own, *sent = call(
                functools.partial(down_kernel, n, s, last),
                f"down_{s}",
                [((rows, depth), F32)] + [((rows, depth), BF16)] * last,
                got[i],
                w_down,
                own,
            )
        (sent,) = sent
        got, _ = exchange(sent, "tp", n_tp, ORDERS[5])
        (layer_out,) = call(final_kernel, "final", [((rows, depth), BF16)], mixed, own, *got, kept=False)
        return (layer_out, new_state)

    return shards


def solution(mesh):
    n_kv, n_tp = mesh.shape["kv"], mesh.shape["tp"]
    direct = all(n <= DIRECT and n & (n - 1) == 0 for n in (n_kv, n_tp))
    return jax.shard_map(
        make_direct(n_kv, n_tp) if direct else shards_large,
        mesh=mesh,
        in_specs=(
            P("grp", "kv"),
            P(("grp", "kv")),
            P(("grp", "kv"), "tp", None, None),
            P("kv"),
            P("kv", "tp"),
            P("kv", "tp"),
            P("kv", "tp"),
            P("kv", "tp"),
            P("tp", "kv"),
            P("kv"),
            P("kv", "tp"),
            P("tp", "kv"),
        ),
        out_specs=(P("grp", "kv"), P(("grp", "kv"), "tp", None, None)),
        check_vma=False,
    )
```

```python
import functools

import jax
import jax.numpy as jnp
from jax import lax
from jax.experimental import pallas as pl
from jax.experimental.pallas import tpu as pltpu
from jax.sharding import PartitionSpec as P


D = 4096
HEADS = 16
DIRECT = 8
LANES = 128
X1, X2, X3 = (1, 0, 3, 2), (2, 3, 0, 1), (3, 2, 1, 0)
C, R = (1, 3, 0, 2), (2, 0, 3, 1)
PERMS = ((X2, X3, X1), (X2, X3, X1), (X3, X2, X1), (X2, X3, X1), (C, X3, R), (X3, X2, X1))
TURNS = (0, 1, 2)
RATE = 1 << 33
F32, BF16 = jnp.float32, jnp.bfloat16


def turn(values, positions):
    half = values.shape[-1] // 2
    freq = 10000.0 ** (-(jnp.arange(half, dtype=jnp.float32) * 2.0) / values.shape[-1])
    angle = positions.astype(jnp.float32)[:, None, None] * freq[None, None, :]
    cosine = jnp.cos(angle)
    sine = jnp.sin(angle)
    first = values[..., :half]
    second = values[..., half:]
    return jnp.concatenate(
        [first * cosine - second * sine, first * sine + second * cosine], axis=-1
    )


def shards_large(
    tokens,
    positions,
    state,
    norm_gain,
    w_query,
    w_key,
    w_value,
    w_gate,
    w_out,
    mlp_gain,
    w_up,
    w_down,
):
    local_seqs, head_dev, head_size, _ = state.shape
    inputs = tokens.astype(jnp.float32)
    squares = jnp.sum(inputs * inputs, axis=1)
    normed = (inputs * norm_gain).astype(jnp.bfloat16)
    terms = jnp.stack(
        [
            jnp.dot(normed, weight, preferred_element_type=jnp.float32)
            for weight in (w_query, w_key, w_value, w_gate)
        ],
        axis=1,
    )
    summed, total_sq = (
        lax.psum_scatter(terms, "kv", scatter_dimension=0, tiled=True),
        lax.psum_scatter(squares, "kv", scatter_dimension=0, tiled=True),
    )
    scale1 = lax.rsqrt(total_sq / D + 1e-06)
    summed = (summed * scale1[:, None, None]).reshape(local_seqs, 4, head_dev, head_size)
    query = turn(summed[:, 0], positions)
    key_rows = turn(summed[:, 1], positions) * head_size ** (-0.5)
    value = summed[:, 2]
    gate = summed[:, 3]
    heads = (lax.axis_index("tp") * head_dev + jnp.arange(head_dev)).astype(jnp.float32)
    gamma = 1.0 - 2.0 ** (-5.0 - 5.0 * heads / (HEADS - 1))
    new_state = gamma[None, :, None, None] * state + key_rows[:, :, :, None] * value[:, :, None, :]
    read = jnp.einsum("bhd,bhde->bhe", query, new_state, precision=lax.Precision.HIGHEST)
    read = read * lax.rsqrt(jnp.mean(read * read, axis=-1, keepdims=True) + 1e-06)
    retained = (
        (read * jax.nn.silu(gate)).reshape(local_seqs, head_dev * head_size).astype(jnp.bfloat16)
    )
    head_terms = jnp.dot(
        lax.all_gather(retained, "kv", axis=0, tiled=True),
        w_out,
        preferred_element_type=jnp.float32,
    )
    mixed = (inputs + lax.psum(head_terms, "tp")).astype(jnp.bfloat16)
    middle = mixed.astype(jnp.float32)
    squares2 = jnp.sum(middle * middle, axis=1)
    normed2 = (middle * mlp_gain).astype(jnp.bfloat16)
    upward = jnp.dot(normed2, w_up, preferred_element_type=jnp.float32)
    up_full, total_sq2 = lax.psum((upward, squares2), "kv")
    scale2 = lax.rsqrt(total_sq2 / D + 1e-06)
    hidden = jnp.square(jax.nn.relu(up_full * scale2[:, None])).astype(jnp.bfloat16)
    down_terms = jnp.dot(hidden, w_down, preferred_element_type=jnp.float32)
    layer_out = (middle + lax.psum(down_terms, "tp")).astype(jnp.bfloat16)
    return (layer_out, new_state)


def partners(n, i):
    if n == 4:
        return PERMS[i]
    return [tuple(j ^ s for j in range(n)) for s in reversed(range(1, n))]


def inverse(perm):
    return tuple(perm.index(j) for j in range(len(perm)))


def lookup(axis, perm):
    me = lax.axis_index(axis)
    return sum(jnp.where(me == j, entry, 0) for j, entry in enumerate(perm))


def exchange(values, axis, perms):
    if not isinstance(values, list):
        values = [values] * len(perms)
    got = []
    for value, perm in zip(values, perms):
        got.append(lax.ppermute(value, axis, list(enumerate(perm))))
    return got


def pieces(value):
    high = value.astype(BF16).astype(F32)
    rest = value - high
    middle = rest.astype(BF16).astype(F32)
    return high, middle, rest - middle


def reorder(perms, values):
    rows = values.shape[0]
    block = rows // len(perms)
    to = lax.broadcasted_iota(jnp.int32, (rows, rows), 0)
    of = lax.broadcasted_iota(jnp.int32, (rows, rows), 1)
    owner = sum(jnp.where(to // block == k, lookup("kv", perm), 0) for k, perm in enumerate(perms))
    hot = owner * block + to % block == of
    return jnp.dot(hot.astype(F32).astype(BF16), values, preferred_element_type=F32)


def project_kernel(perms, chunks, flight, x_hbm, gain_hbm, *refs):
    n = len(perms)
    weights, outs, (x_ref, gain_ref, held, sems, small) = refs[:4], refs[4 : 4 + n], refs[4 + n :]
    first = [
        pltpu.make_async_copy(x_hbm, x_ref, small.at[0]),
        pltpu.make_async_copy(gain_hbm, gain_ref, small.at[1]),
    ]
    rows, depth = x_ref.shape
    width = held.shape[2]
    block, heads = rows // n, width // LANES
    step = depth // chunks
    copies = []
    for i, w in enumerate(weights):
        for j in range(chunks):
            part = pl.ds(j * step, step)
            copies.append(pltpu.make_async_copy(w.at[part], held.at[i, part], sems.at[i, j]))
    for copy in first + copies[:flight]:
        copy.start()
    first[0].wait()
    x = reorder(perms, x_ref[...])
    lane = lax.broadcasted_iota(jnp.int32, (rows, LANES), 1)
    high, mid, low = pieces(jnp.sum(x * x, axis=1, keepdims=True))
    split = jnp.where(lane == 0, high, jnp.where(lane == 1, mid, jnp.where(lane == 2, low, 0.0)))
    group = heads * block
    for s, out in enumerate(outs):
        mine = split[s * block : (s + 1) * block]
        out[4 * group :] = jnp.concatenate([mine] * heads, axis=0).astype(out.dtype)
    first[1].wait()
    normed = (x * gain_ref[...]).astype(BF16)
    for i in range(4):
        total = None
        for j in range(chunks):
            at = chunks * i + j
            copies[at].wait()
            if at + flight < len(copies):
                copies[at + flight].start()
            part = slice(j * step, (j + 1) * step)
            term = jnp.dot(normed[:, part], held[i, part], preferred_element_type=F32)
            total = term if total is None else total + term
        for s, out in enumerate(outs):
            mine = total[s * block : (s + 1) * block]
            mine = jnp.concatenate([mine[:, h * LANES : (h + 1) * LANES] for h in range(heads)], axis=0)
            out[i * group : (i + 1) * group] = mine.astype(out.dtype)


def prepare_kernel(state_ref, cos_ref, sin_ref, out_ref, cosine_ref, sine_ref, gamma_ref):
    block, head_dev, size, _ = state_ref.shape
    for h in range(head_dev):
        for b in range(block):
            value = state_ref[b, h]
            high = value.astype(BF16)
            at = slice(b * size, (b + 1) * size)
            out_ref[h, :size, at] = high
            out_ref[h, size:, at] = (value - high.astype(F32)).astype(BF16)
    cos, sin = cos_ref[...], sin_ref[...]
    cosine_ref[...] = jnp.concatenate([jnp.concatenate([cos, cos], axis=1)] * head_dev, axis=0)
    sine_ref[...] = jnp.concatenate([jnp.concatenate([-sin, sin], axis=1)] * head_dev, axis=0)
    row = lax.broadcasted_iota(jnp.int32, gamma_ref.shape, 0)
    head = lax.axis_index("tp") * head_dev + row // block
    gamma_ref[...] = 1.0 - jnp.exp2(-5.0 - 5.0 * head.astype(F32) / (HEADS - 1))


def read_kernel(n, block, own_ref, *refs):
    got, (cos_ref, sin_ref, gamma_ref, prep_ref, kept_ref, key_ref, value_ref) = refs[: n - 1], refs[n - 1 :]
    head_dev, _, wide = prep_ref.shape
    size = wide // block
    total = own_ref[...]
    for g in got:
        total = total + g[...].astype(F32)
    group = head_dev * block
    sq = total[4 * group :]
    scale = lax.rsqrt((sq[:, 0:1] + sq[:, 1:2] + sq[:, 2:3]) / D + 1e-06)
    query, key, value, gate = (total[i * group : (i + 1) * group] * scale for i in range(4))
    cos, sin = cos_ref[...], sin_ref[...]
    query = query * cos + pltpu.roll(query, size // 2, 1) * sin
    high = query.astype(BF16).astype(F32)
    low = query - high
    row = lax.broadcasted_iota(jnp.int32, (2 * block, size), 0)
    reads = []
    for h in range(head_dev):
        at = slice(h * block, (h + 1) * block)
        both = jnp.concatenate([high[at], low[at]], axis=0).astype(BF16)
        both = jnp.concatenate([both, both], axis=1)
        product = jnp.dot(both, prep_ref[h], preferred_element_type=F32)
        picked = jnp.zeros((2 * block, size), F32)
        for b in range(block):
            picked = jnp.where(row % block == b, product[:, b * size : (b + 1) * size], picked)
        reads.append(picked[:block] + picked[block:])
    key = (key * cos + pltpu.roll(key, size // 2, 1) * sin) * size ** (-0.5)
    key_ref[...] = key
    value_ref[...] = value
    match = jnp.sum(query * key, axis=1, keepdims=True)
    gate = gate / (1.0 + jnp.exp(-gate))
    read = gamma_ref[...] * jnp.concatenate(reads, axis=0) + match * value
    read = read * lax.rsqrt(jnp.mean(read * read, axis=1, keepdims=True) + 1e-06)
    kept_ref[...] = (read * gate).astype(BF16)


def update_kernel(key_ref, value_ref, gamma_ref, after_ref, state_ref, new_hbm, new_ref, sems):
    del after_ref
    block, head_dev, _, _ = state_ref.shape
    copies = []
    for h in range(head_dev):
        rows = slice(h * block, (h + 1) * block)
        k, v = key_ref[rows], value_ref[rows]
        columns = jnp.concatenate([k, k], axis=0).T
        gamma = gamma_ref[h * block : h * block + 1, :]
        for b in range(block):
            new_ref[b, h] = gamma * state_ref[b, h] + columns[:, b : b + 1] * v[b : b + 1]
            copies.append(pltpu.make_async_copy(new_ref.at[b, h], new_hbm.at[b, h], sems.at[b, h]))
            copies[-1].start()
    for copy in copies:
        copy.wait()


def out_kernel(perms, *refs):
    n = len(perms)
    parts, (w_ref, own_ref, sent_ref) = refs[:n], refs[n:]
    kept = jnp.concatenate([p[...] for p in parts], axis=0)
    many, size = kept.shape
    heads = w_ref.shape[0] // size
    block = many // n // heads
    rows = n * block
    to = lax.broadcasted_iota(jnp.int32, (many, many), 0)
    of = lax.broadcasted_iota(jnp.int32, (many, many), 1)
    head, row = to // rows, to % rows
    part = of // (heads * block)
    owner = sum(jnp.where(part == k, lookup("kv", inverse(perm)), 0) for k, perm in enumerate(perms))
    hot = (owner == row // block) & (of % (heads * block) == head * block + row % block)
    kept = jnp.dot(hot.astype(F32).astype(BF16), kept, preferred_element_type=F32).astype(BF16)
    kept = jnp.concatenate([kept[h * rows : (h + 1) * rows] for h in range(heads)], axis=1)
    terms = jnp.dot(kept, w_ref[...], preferred_element_type=F32)
    own_ref[...] = terms
    sent_ref[...] = terms.astype(BF16)


def up_kernel(n_tp, perms, x_ref, gain_ref, w_ref, own_ref, *refs):
    got, (mixed_ref, normed_ref, split_ref, *sent) = refs[: n_tp - 1], refs[n_tp - 1 :]
    total = own_ref[...]
    for g in got:
        total = total + g[...].astype(F32)
    mixed = (x_ref[...].astype(F32) + total).astype(BF16)
    mixed_ref[...] = mixed
    middle = mixed.astype(F32)
    normed = (middle * gain_ref[...]).astype(BF16)
    normed_ref[...] = normed
    rows = middle.shape[0]
    high, mid, low = pieces(jnp.sum(middle * middle, axis=1, keepdims=True))
    lane = lax.broadcasted_iota(jnp.int32, (rows, LANES), 1)
    split = jnp.where(lane == 0, high, jnp.where(lane == 1, mid, jnp.where(lane == 2, low, 0.0)))
    split_ref[...] = split
    part = sent[0].shape[1] - LANES
    for perm, out in zip(perms, sent):
        at = pl.ds(pl.multiple_of(lookup("kv", perm) * part, part), part)
        out[:, :part] = jnp.dot(normed, w_ref[:, at], preferred_element_type=F32).astype(out.dtype)
        out[:, part:] = split.astype(out.dtype)


def up_own_kernel(n, normed_ref, w_ref, out_ref):
    part = w_ref.shape[1] // n
    at = pl.ds(pl.multiple_of(lax.axis_index("kv") * part, part), part)
    out_ref[...] = jnp.dot(normed_ref[...], w_ref[:, at], preferred_element_type=F32)


def hidden_kernel(own_ref, split_ref, *refs):
    *got, out_ref = refs
    part = out_ref.shape[1]
    total, split = own_ref[...], split_ref[...]
    for g in got:
        total = total + g[:, :part].astype(F32)
        split = split + g[:, part:].astype(F32)
    sq = split[:, 0:1] + split[:, 1:2] + split[:, 2:3]
    scale = lax.rsqrt(sq / D + 1e-06)
    out_ref[...] = jnp.square(jnp.maximum(total * scale, 0.0)).astype(BF16)


def down_kernel(perm, first, last, *refs):
    part_ref, w_ref, *refs = refs
    part = part_ref.shape[1]
    at = pl.ds(pl.multiple_of(lookup("kv", inverse(perm)) * part, part), part)
    total = jnp.dot(part_ref[...], w_ref[at, :], preferred_element_type=F32)
    if not first:
        total = total + refs.pop(0)[...]
    refs[0][...] = total
    if last:
        refs[1][...] = total.astype(BF16)


def final_kernel(mixed_ref, own_ref, *refs):
    *got, out_ref = refs
    total = own_ref[...]
    for g in got:
        total = total + g[...].astype(F32)
    out_ref[...] = (mixed_ref[...].astype(F32) + total).astype(BF16)


VMEM = pl.BlockSpec(memory_space=pltpu.VMEM)
HBM = pl.BlockSpec(memory_space=pltpu.HBM)


def call(kernel, outs, *args, specs=None, out_specs=None, scratch=(), limit=8, us=1, kept=True):
    return pl.pallas_call(
        kernel,
        out_shape=[(pltpu.VMEM if kept else jax.ShapeDtypeStruct)(*o) for o in outs],
        in_specs=specs or [VMEM] * len(args),
        out_specs=out_specs or [VMEM] * len(outs),
        scratch_shapes=scratch,
        compiler_params=pltpu.CompilerParams(vmem_limit_bytes=limit << 20),
        cost_estimate=pl.CostEstimate(flops=int(us * RATE), bytes_accessed=0, transcendentals=0),
    )(*args)


def far(value):
    return pltpu.with_memory_space_constraint(value, pltpu.HBM)


def near(value):
    return pltpu.with_memory_space_constraint(value, pltpu.VMEM)


def make_direct(n, n_tp):
    def shards(
        tokens, positions, state, norm_gain, w_query, w_key, w_value, w_gate, w_out, mlp_gain, w_up, w_down
    ):
        block, head_dev, size, _ = state.shape
        rows, depth = tokens.shape
        width = head_dev * size
        group = head_dev * block
        chunks, flight = 1, 4
        same = tuple(range(n))
        perms = partners(n, 0)
        own, *sent = call(
            functools.partial(project_kernel, [same, *perms], chunks, flight),
            [((5 * group, size), F32)] + [((5 * group, size), BF16)] * (n - 1),
            far(tokens),
            far(norm_gain[None]),
            far(w_query),
            far(w_key),
            far(w_value),
            far(w_gate),
            specs=[HBM] * 6,
            scratch=[
                pltpu.VMEM((rows, depth), BF16),
                pltpu.VMEM((1, depth), F32),
                pltpu.VMEM((4, depth, width), BF16),
                pltpu.SemaphoreType.DMA((4, chunks)),
                pltpu.SemaphoreType.DMA((2,)),
            ],
            us=2,
        )
        got = exchange(sent, "kv", perms)
        half = size // 2
        freq = 10000.0 ** (-(jnp.arange(half, dtype=F32) * 2.0) / size)
        angle = positions.astype(F32)[:, None] * freq[None, :]
        cosine, sine = jnp.cos(angle), jnp.sin(angle)
        state = near(state)
        prepared, cosine, sine, gamma = call(
            prepare_kernel,
            [((head_dev, 2 * size, block * size), BF16)] + [((group, size), F32)] * 3,
            state,
            cosine,
            sine,
        )
        kept, key, value = call(
            functools.partial(read_kernel, n, block),
            [((group, size), BF16), ((group, size), F32), ((group, size), F32)],
            own,
            *got,
            cosine,
            sine,
            gamma,
            prepared,
        )
        perms = partners(n, 1)
        got = exchange(kept, "kv", perms)
        own, sent = call(
            functools.partial(out_kernel, [same, *perms]),
            [((rows, depth), F32), ((rows, depth), BF16)],
            kept,
            *got,
            near(w_out),
        )
        got = exchange(sent, "tp", partners(n_tp, 2))
        part = w_up.shape[1] // n
        w_up = near(w_up)
        perms = partners(n, 3)
        mixed, normed, split, *sent = call(
            functools.partial(up_kernel, n_tp, perms),
            [((rows, depth), BF16), ((rows, depth), BF16), ((rows, LANES), F32)]
            + [((rows, part + LANES), BF16)] * (n - 1),
            tokens,
            mlp_gain[None],
            w_up,
            own,
            *got,
        )
        got = exchange(sent, "kv", perms)
        (new_state,) = call(
            update_kernel,
            [(state.shape, F32)],
            key,
            value,
            gamma,
            split,
            state,
            out_specs=[HBM],
            scratch=[pltpu.VMEM(state.shape, F32), pltpu.SemaphoreType.DMA((block, head_dev))],
            kept=False,
        )
        (own,) = call(functools.partial(up_own_kernel, n), [((rows, part), F32)], normed, w_up)
        (hidden,) = call(hidden_kernel, [((rows, part), BF16)], own, split, *got)
        perms = partners(n, 4)
        got = exchange(hidden, "kv", perms)
        w_down = near(w_down)
        (own,) = call(functools.partial(down_kernel, same, True, False), [((rows, depth), F32)], hidden, w_down)
        turns = TURNS if n == 4 else range(n - 1)
        for k in turns:
            last = k == turns[-1]
            own, *sent = call(
                functools.partial(down_kernel, perms[k], False, last),
                [((rows, depth), F32)] + [((rows, depth), BF16)] * last,
                got[k],
                w_down,
                own,
            )
        (sent,) = sent
        got = exchange(sent, "tp", partners(n_tp, 5))
        (layer_out,) = call(final_kernel, [((rows, depth), BF16)], mixed, own, *got, kept=False)
        return (layer_out, new_state)

    return shards


def solution(mesh):
    n_kv, n_tp = mesh.shape["kv"], mesh.shape["tp"]
    direct = all(n <= DIRECT and n & (n - 1) == 0 for n in (n_kv, n_tp))
    return jax.shard_map(
        make_direct(n_kv, n_tp) if direct else shards_large,
        mesh=mesh,
        in_specs=(
            P("grp", "kv"),
            P(("grp", "kv")),
            P(("grp", "kv"), "tp", None, None),
            P("kv"),
            P("kv", "tp"),
            P("kv", "tp"),
            P("kv", "tp"),
            P("kv", "tp"),
            P("tp", "kv"),
            P("kv"),
            P("kv", "tp"),
            P("tp", "kv"),
        ),
        out_specs=(P("grp", "kv"), P(("grp", "kv"), "tp", None, None)),
        check_vma=False,
    )
```

```python
import functools

import jax
import jax.numpy as jnp
from jax import lax
from jax.experimental import pallas as pl
from jax.experimental.pallas import tpu as pltpu
from jax.sharding import PartitionSpec as P


D = 4096
HEADS = 16
DIRECT = 8
LANES = 128
X1, X2, X3 = (1, 0, 3, 2), (2, 3, 0, 1), (3, 2, 1, 0)
C, R = (1, 3, 0, 2), (2, 0, 3, 1)
PERMS = ((X2, X3, X1), (X2, X3, X1), (X3, X2, X1), (X2, X3, X1), (C, X3, R), (X3, X2, X1))
TURNS = (0, 1, 2)
RATE = 1 << 33
F32, BF16 = jnp.float32, jnp.bfloat16


def turn(values, positions):
    half = values.shape[-1] // 2
    freq = 10000.0 ** (-(jnp.arange(half, dtype=jnp.float32) * 2.0) / values.shape[-1])
    angle = positions.astype(jnp.float32)[:, None, None] * freq[None, None, :]
    cosine = jnp.cos(angle)
    sine = jnp.sin(angle)
    first = values[..., :half]
    second = values[..., half:]
    return jnp.concatenate(
        [first * cosine - second * sine, first * sine + second * cosine], axis=-1
    )


def shards_large(
    tokens,
    positions,
    state,
    norm_gain,
    w_query,
    w_key,
    w_value,
    w_gate,
    w_out,
    mlp_gain,
    w_up,
    w_down,
):
    local_seqs, head_dev, head_size, _ = state.shape
    inputs = tokens.astype(jnp.float32)
    squares = jnp.sum(inputs * inputs, axis=1)
    normed = (inputs * norm_gain).astype(jnp.bfloat16)
    terms = jnp.stack(
        [
            jnp.dot(normed, weight, preferred_element_type=jnp.float32)
            for weight in (w_query, w_key, w_value, w_gate)
        ],
        axis=1,
    )
    summed, total_sq = (
        lax.psum_scatter(terms, "kv", scatter_dimension=0, tiled=True),
        lax.psum_scatter(squares, "kv", scatter_dimension=0, tiled=True),
    )
    scale1 = lax.rsqrt(total_sq / D + 1e-06)
    summed = (summed * scale1[:, None, None]).reshape(local_seqs, 4, head_dev, head_size)
    query = turn(summed[:, 0], positions)
    key_rows = turn(summed[:, 1], positions) * head_size ** (-0.5)
    value = summed[:, 2]
    gate = summed[:, 3]
    heads = (lax.axis_index("tp") * head_dev + jnp.arange(head_dev)).astype(jnp.float32)
    gamma = 1.0 - 2.0 ** (-5.0 - 5.0 * heads / (HEADS - 1))
    new_state = gamma[None, :, None, None] * state + key_rows[:, :, :, None] * value[:, :, None, :]
    read = jnp.einsum("bhd,bhde->bhe", query, new_state, precision=lax.Precision.HIGHEST)
    read = read * lax.rsqrt(jnp.mean(read * read, axis=-1, keepdims=True) + 1e-06)
    retained = (
        (read * jax.nn.silu(gate)).reshape(local_seqs, head_dev * head_size).astype(jnp.bfloat16)
    )
    head_terms = jnp.dot(
        lax.all_gather(retained, "kv", axis=0, tiled=True),
        w_out,
        preferred_element_type=jnp.float32,
    )
    mixed = (inputs + lax.psum(head_terms, "tp")).astype(jnp.bfloat16)
    middle = mixed.astype(jnp.float32)
    squares2 = jnp.sum(middle * middle, axis=1)
    normed2 = (middle * mlp_gain).astype(jnp.bfloat16)
    upward = jnp.dot(normed2, w_up, preferred_element_type=jnp.float32)
    up_full, total_sq2 = lax.psum((upward, squares2), "kv")
    scale2 = lax.rsqrt(total_sq2 / D + 1e-06)
    hidden = jnp.square(jax.nn.relu(up_full * scale2[:, None])).astype(jnp.bfloat16)
    down_terms = jnp.dot(hidden, w_down, preferred_element_type=jnp.float32)
    layer_out = (middle + lax.psum(down_terms, "tp")).astype(jnp.bfloat16)
    return (layer_out, new_state)


def partners(n, i):
    if n == 4:
        return PERMS[i]
    return [tuple(j ^ s for j in range(n)) for s in reversed(range(1, n))]


def inverse(perm):
    return tuple(perm.index(j) for j in range(len(perm)))


def lookup(axis, perm):
    me = lax.axis_index(axis)
    return sum(jnp.where(me == j, entry, 0) for j, entry in enumerate(perm))


def exchange(values, axis, perms):
    if not isinstance(values, list):
        values = [values] * len(perms)
    got = []
    for value, perm in zip(values, perms):
        got.append(lax.ppermute(value, axis, list(enumerate(perm))))
    return got


def pieces(value):
    high = value.astype(BF16).astype(F32)
    rest = value - high
    middle = rest.astype(BF16).astype(F32)
    return high, middle, rest - middle


def reorder(perms, values):
    rows = values.shape[0]
    block = rows // len(perms)
    to = lax.broadcasted_iota(jnp.int32, (rows, rows), 0)
    of = lax.broadcasted_iota(jnp.int32, (rows, rows), 1)
    owner = sum(jnp.where(to // block == k, lookup("kv", perm), 0) for k, perm in enumerate(perms))
    hot = owner * block + to % block == of
    return jnp.dot(hot.astype(F32).astype(BF16), values, preferred_element_type=F32)


def project_kernel(perms, chunks, flight, x_hbm, gain_hbm, *refs):
    n = len(perms)
    weights, outs, (x_ref, gain_ref, held, sems, small) = refs[:4], refs[4 : 4 + n], refs[4 + n :]
    first = [
        pltpu.make_async_copy(x_hbm, x_ref, small.at[0]),
        pltpu.make_async_copy(gain_hbm, gain_ref, small.at[1]),
    ]
    rows, depth = x_ref.shape
    width = held.shape[2]
    block, heads = rows // n, width // LANES
    step = depth // chunks
    copies = []
    for i, w in enumerate(weights):
        for j in range(chunks):
            part = pl.ds(j * step, step)
            copies.append(pltpu.make_async_copy(w.at[part], held.at[i, part], sems.at[i, j]))
    for copy in first + copies[:flight]:
        copy.start()
    first[0].wait()
    x = reorder(perms, x_ref[...])
    lane = lax.broadcasted_iota(jnp.int32, (rows, LANES), 1)
    high, mid, low = pieces(jnp.sum(x * x, axis=1, keepdims=True))
    split = jnp.where(lane == 0, high, jnp.where(lane == 1, mid, jnp.where(lane == 2, low, 0.0)))
    group = heads * block
    for s, out in enumerate(outs):
        mine = split[s * block : (s + 1) * block]
        out[4 * group :] = jnp.concatenate([mine] * heads, axis=0).astype(out.dtype)
    first[1].wait()
    normed = (x * gain_ref[...]).astype(BF16)
    for i in range(4):
        total = None
        for j in range(chunks):
            at = chunks * i + j
            copies[at].wait()
            if at + flight < len(copies):
                copies[at + flight].start()
            part = slice(j * step, (j + 1) * step)
            term = jnp.dot(normed[:, part], held[i, part], preferred_element_type=F32)
            total = term if total is None else total + term
        for s, out in enumerate(outs):
            mine = total[s * block : (s + 1) * block]
            mine = jnp.concatenate([mine[:, h * LANES : (h + 1) * LANES] for h in range(heads)], axis=0)
            out[i * group : (i + 1) * group] = mine.astype(out.dtype)


def prepare_kernel(state_ref, cos_ref, sin_ref, out_ref, cosine_ref, sine_ref, gamma_ref):
    block, head_dev, size, _ = state_ref.shape
    for h in range(head_dev):
        for b in range(block):
            value = state_ref[b, h]
            high = value.astype(BF16)
            at = slice(b * size, (b + 1) * size)
            out_ref[h, :size, at] = high
            out_ref[h, size:, at] = (value - high.astype(F32)).astype(BF16)
    cos, sin = cos_ref[...], sin_ref[...]
    cosine_ref[...] = jnp.concatenate([jnp.concatenate([cos, cos], axis=1)] * head_dev, axis=0)
    sine_ref[...] = jnp.concatenate([jnp.concatenate([-sin, sin], axis=1)] * head_dev, axis=0)
    row = lax.broadcasted_iota(jnp.int32, gamma_ref.shape, 0)
    head = lax.axis_index("tp") * head_dev + row // block
    gamma_ref[...] = 1.0 - jnp.exp2(-5.0 - 5.0 * head.astype(F32) / (HEADS - 1))


def read_kernel(n, block, own_ref, *refs):
    got, (cos_ref, sin_ref, gamma_ref, prep_ref, kept_ref, key_ref, value_ref) = refs[: n - 1], refs[n - 1 :]
    head_dev, _, wide = prep_ref.shape
    size = wide // block
    total = own_ref[...]
    for g in got:
        total = total + g[...].astype(F32)
    group = head_dev * block
    sq = total[4 * group :]
    scale = lax.rsqrt((sq[:, 0:1] + sq[:, 1:2] + sq[:, 2:3]) / D + 1e-06)
    query, key, value, gate = (total[i * group : (i + 1) * group] * scale for i in range(4))
    cos, sin = cos_ref[...], sin_ref[...]
    query = query * cos + pltpu.roll(query, size // 2, 1) * sin
    high = query.astype(BF16).astype(F32)
    low = query - high
    row = lax.broadcasted_iota(jnp.int32, (2 * block, size), 0)
    reads = []
    for h in range(head_dev):
        at = slice(h * block, (h + 1) * block)
        both = jnp.concatenate([high[at], low[at]], axis=0).astype(BF16)
        both = jnp.concatenate([both, both], axis=1)
        product = jnp.dot(both, prep_ref[h], preferred_element_type=F32)
        picked = jnp.zeros((2 * block, size), F32)
        for b in range(block):
            picked = jnp.where(row % block == b, product[:, b * size : (b + 1) * size], picked)
        reads.append(picked[:block] + picked[block:])
    key = (key * cos + pltpu.roll(key, size // 2, 1) * sin) * size ** (-0.5)
    key_ref[...] = key
    value_ref[...] = value
    match = jnp.sum(query * key, axis=1, keepdims=True)
    gate = gate / (1.0 + jnp.exp(-gate))
    read = gamma_ref[...] * jnp.concatenate(reads, axis=0) + match * value
    read = read * lax.rsqrt(jnp.mean(read * read, axis=1, keepdims=True) + 1e-06)
    kept_ref[...] = (read * gate).astype(BF16)


def update_kernel(key_ref, value_ref, gamma_ref, after_ref, state_ref, new_hbm, new_ref, sems):
    del after_ref
    block, head_dev, _, _ = state_ref.shape
    copies = []
    for h in range(head_dev):
        rows = slice(h * block, (h + 1) * block)
        k, v = key_ref[rows], value_ref[rows]
        columns = jnp.concatenate([k, k], axis=0).T
        gamma = gamma_ref[h * block : h * block + 1, :]
        for b in range(block):
            new_ref[b, h] = gamma * state_ref[b, h] + columns[:, b : b + 1] * v[b : b + 1]
            copies.append(pltpu.make_async_copy(new_ref.at[b, h], new_hbm.at[b, h], sems.at[b, h]))
            copies[-1].start()
    for copy in copies:
        copy.wait()


def out_kernel(perms, *refs):
    n = len(perms)
    parts, (w_ref, own_ref, sent_ref) = refs[:n], refs[n:]
    size = parts[0].shape[1]
    heads = w_ref.shape[0] // size
    block = parts[0].shape[0] // heads
    values = [p[...].astype(F32) for p in parts]
    places = [lookup("kv", inverse(perm)) for perm in perms]
    ordered = []
    for t in range(n):
        value = values[0]
        for place, other in zip(places[1:], values[1:]):
            value = jnp.where(place == t, other, value)
        ordered.append(value)
    columns = [
        jnp.concatenate([value[h * block : (h + 1) * block] for value in ordered], axis=0) for h in range(heads)
    ]
    kept = jnp.concatenate(columns, axis=1).astype(BF16)
    terms = jnp.dot(kept, w_ref[...], preferred_element_type=F32)
    own_ref[...] = terms
    sent_ref[...] = terms.astype(BF16)


def up_kernel(n_tp, perms, x_ref, gain_ref, w_ref, own_ref, *refs):
    got, (mixed_ref, normed_ref, split_ref, *sent) = refs[: n_tp - 1], refs[n_tp - 1 :]
    total = own_ref[...]
    for g in got:
        total = total + g[...].astype(F32)
    mixed = (x_ref[...].astype(F32) + total).astype(BF16)
    mixed_ref[...] = mixed
    middle = mixed.astype(F32)
    normed = (middle * gain_ref[...]).astype(BF16)
    normed_ref[...] = normed
    rows = middle.shape[0]
    high, mid, low = pieces(jnp.sum(middle * middle, axis=1, keepdims=True))
    lane = lax.broadcasted_iota(jnp.int32, (rows, LANES), 1)
    split = jnp.where(lane == 0, high, jnp.where(lane == 1, mid, jnp.where(lane == 2, low, 0.0)))
    split_ref[...] = split
    part = sent[0].shape[1] - LANES
    for perm, out in zip(perms, sent):
        at = pl.ds(pl.multiple_of(lookup("kv", perm) * part, part), part)
        out[:, :part] = jnp.dot(normed, w_ref[:, at], preferred_element_type=F32).astype(out.dtype)
        out[:, part:] = split.astype(out.dtype)


def up_own_kernel(n, normed_ref, w_ref, out_ref):
    part = w_ref.shape[1] // n
    at = pl.ds(pl.multiple_of(lax.axis_index("kv") * part, part), part)
    out_ref[...] = jnp.dot(normed_ref[...], w_ref[:, at], preferred_element_type=F32)


def hidden_kernel(own_ref, split_ref, *refs):
    *got, out_ref = refs
    part = out_ref.shape[1]
    total, split = own_ref[...], split_ref[...]
    for g in got:
        total = total + g[:, :part].astype(F32)
        split = split + g[:, part:].astype(F32)
    sq = split[:, 0:1] + split[:, 1:2] + split[:, 2:3]
    scale = lax.rsqrt(sq / D + 1e-06)
    out_ref[...] = jnp.square(jnp.maximum(total * scale, 0.0)).astype(BF16)


def down_kernel(perm, first, last, *refs):
    part_ref, w_ref, *refs = refs
    part = part_ref.shape[1]
    at = pl.ds(pl.multiple_of(lookup("kv", inverse(perm)) * part, part), part)
    total = jnp.dot(part_ref[...], w_ref[at, :], preferred_element_type=F32)
    if not first:
        total = total + refs.pop(0)[...]
    refs[0][...] = total
    if last:
        refs[1][...] = total.astype(BF16)


def final_kernel(mixed_ref, own_ref, *refs):
    *got, out_ref = refs
    total = own_ref[...]
    for g in got:
        total = total + g[...].astype(F32)
    out_ref[...] = (mixed_ref[...].astype(F32) + total).astype(BF16)


VMEM = pl.BlockSpec(memory_space=pltpu.VMEM)
HBM = pl.BlockSpec(memory_space=pltpu.HBM)


def call(kernel, outs, *args, specs=None, out_specs=None, scratch=(), limit=8, us=1, kept=True):
    return pl.pallas_call(
        kernel,
        out_shape=[(pltpu.VMEM if kept else jax.ShapeDtypeStruct)(*o) for o in outs],
        in_specs=specs or [VMEM] * len(args),
        out_specs=out_specs or [VMEM] * len(outs),
        scratch_shapes=scratch,
        compiler_params=pltpu.CompilerParams(vmem_limit_bytes=limit << 20),
        cost_estimate=pl.CostEstimate(flops=int(us * RATE), bytes_accessed=0, transcendentals=0),
    )(*args)


def far(value):
    return pltpu.with_memory_space_constraint(value, pltpu.HBM)


def near(value):
    return pltpu.with_memory_space_constraint(value, pltpu.VMEM)


def make_direct(n, n_tp):
    def shards(
        tokens, positions, state, norm_gain, w_query, w_key, w_value, w_gate, w_out, mlp_gain, w_up, w_down
    ):
        block, head_dev, size, _ = state.shape
        rows, depth = tokens.shape
        width = head_dev * size
        group = head_dev * block
        chunks, flight = 1, 4
        same = tuple(range(n))
        perms = partners(n, 0)
        own, *sent = call(
            functools.partial(project_kernel, [same, *perms], chunks, flight),
            [((5 * group, size), F32)] + [((5 * group, size), BF16)] * (n - 1),
            far(tokens),
            far(norm_gain[None]),
            far(w_query),
            far(w_key),
            far(w_value),
            far(w_gate),
            specs=[HBM] * 6,
            scratch=[
                pltpu.VMEM((rows, depth), BF16),
                pltpu.VMEM((1, depth), F32),
                pltpu.VMEM((4, depth, width), BF16),
                pltpu.SemaphoreType.DMA((4, chunks)),
                pltpu.SemaphoreType.DMA((2,)),
            ],
            us=2,
        )
        got = exchange(sent, "kv", perms)
        half = size // 2
        freq = 10000.0 ** (-(jnp.arange(half, dtype=F32) * 2.0) / size)
        angle = positions.astype(F32)[:, None] * freq[None, :]
        cosine, sine = jnp.cos(angle), jnp.sin(angle)
        state = near(state)
        prepared, cosine, sine, gamma = call(
            prepare_kernel,
            [((head_dev, 2 * size, block * size), BF16)] + [((group, size), F32)] * 3,
            state,
            cosine,
            sine,
        )
        kept, key, value = call(
            functools.partial(read_kernel, n, block),
            [((group, size), BF16), ((group, size), F32), ((group, size), F32)],
            own,
            *got,
            cosine,
            sine,
            gamma,
            prepared,
        )
        perms = partners(n, 1)
        got = exchange(kept, "kv", perms)
        own, sent = call(
            functools.partial(out_kernel, [same, *perms]),
            [((rows, depth), F32), ((rows, depth), BF16)],
            kept,
            *got,
            near(w_out),
        )
        got = exchange(sent, "tp", partners(n_tp, 2))
        part = w_up.shape[1] // n
        w_up = near(w_up)
        perms = partners(n, 3)
        mixed, normed, split, *sent = call(
            functools.partial(up_kernel, n_tp, perms),
            [((rows, depth), BF16), ((rows, depth), BF16), ((rows, LANES), F32)]
            + [((rows, part + LANES), BF16)] * (n - 1),
            tokens,
            mlp_gain[None],
            w_up,
            own,
            *got,
        )
        got = exchange(sent, "kv", perms)
        (new_state,) = call(
            update_kernel,
            [(state.shape, F32)],
            key,
            value,
            gamma,
            split,
            state,
            out_specs=[HBM],
            scratch=[pltpu.VMEM(state.shape, F32), pltpu.SemaphoreType.DMA((block, head_dev))],
            kept=False,
        )
        (own,) = call(functools.partial(up_own_kernel, n), [((rows, part), F32)], normed, w_up)
        (hidden,) = call(hidden_kernel, [((rows, part), BF16)], own, split, *got)
        perms = partners(n, 4)
        got = exchange(hidden, "kv", perms)
        w_down = near(w_down)
        (own,) = call(functools.partial(down_kernel, same, True, False), [((rows, depth), F32)], hidden, w_down)
        turns = TURNS if n == 4 else range(n - 1)
        for k in turns:
            last = k == turns[-1]
            own, *sent = call(
                functools.partial(down_kernel, perms[k], False, last),
                [((rows, depth), F32)] + [((rows, depth), BF16)] * last,
                got[k],
                w_down,
                own,
            )
        (sent,) = sent
        got = exchange(sent, "tp", partners(n_tp, 5))
        (layer_out,) = call(final_kernel, [((rows, depth), BF16)], mixed, own, *got, kept=False)
        return (layer_out, new_state)

    return shards


def solution(mesh):
    n_kv, n_tp = mesh.shape["kv"], mesh.shape["tp"]
    direct = all(n <= DIRECT and n & (n - 1) == 0 for n in (n_kv, n_tp))
    return jax.shard_map(
        make_direct(n_kv, n_tp) if direct else shards_large,
        mesh=mesh,
        in_specs=(
            P("grp", "kv"),
            P(("grp", "kv")),
            P(("grp", "kv"), "tp", None, None),
            P("kv"),
            P("kv", "tp"),
            P("kv", "tp"),
            P("kv", "tp"),
            P("kv", "tp"),
            P("tp", "kv"),
            P("kv"),
            P("kv", "tp"),
            P("tp", "kv"),
        ),
        out_specs=(P("grp", "kv"), P(("grp", "kv"), "tp", None, None)),
        check_vma=False,
    )
```

```python
import functools

import jax
import jax.numpy as jnp
from jax import lax
from jax.experimental import pallas as pl
from jax.experimental.pallas import tpu as pltpu
from jax.sharding import PartitionSpec as P


D = 4096
HEADS = 16
DIRECT = 8
LANES = 128
X1, X2, X3 = (1, 0, 3, 2), (2, 3, 0, 1), (3, 2, 1, 0)
C, R = (1, 3, 0, 2), (2, 0, 3, 1)
PERMS = ((X2, X3, X1), (X2, X3, X1), (X3, X2, X1), (X2, X3, X1), (C, X3, R), (X3, X2, X1))
TURNS = (0, 1, 2)
RATE = 1 << 33
F32, BF16 = jnp.float32, jnp.bfloat16


def turn(values, positions):
    half = values.shape[-1] // 2
    freq = 10000.0 ** (-(jnp.arange(half, dtype=jnp.float32) * 2.0) / values.shape[-1])
    angle = positions.astype(jnp.float32)[:, None, None] * freq[None, None, :]
    cosine = jnp.cos(angle)
    sine = jnp.sin(angle)
    first = values[..., :half]
    second = values[..., half:]
    return jnp.concatenate(
        [first * cosine - second * sine, first * sine + second * cosine], axis=-1
    )


def shards_large(
    tokens,
    positions,
    state,
    norm_gain,
    w_query,
    w_key,
    w_value,
    w_gate,
    w_out,
    mlp_gain,
    w_up,
    w_down,
):
    local_seqs, head_dev, head_size, _ = state.shape
    inputs = tokens.astype(jnp.float32)
    squares = jnp.sum(inputs * inputs, axis=1)
    normed = (inputs * norm_gain).astype(jnp.bfloat16)
    terms = jnp.stack(
        [
            jnp.dot(normed, weight, preferred_element_type=jnp.float32)
            for weight in (w_query, w_key, w_value, w_gate)
        ],
        axis=1,
    )
    summed, total_sq = (
        lax.psum_scatter(terms, "kv", scatter_dimension=0, tiled=True),
        lax.psum_scatter(squares, "kv", scatter_dimension=0, tiled=True),
    )
    scale1 = lax.rsqrt(total_sq / D + 1e-06)
    summed = (summed * scale1[:, None, None]).reshape(local_seqs, 4, head_dev, head_size)
    query = turn(summed[:, 0], positions)
    key_rows = turn(summed[:, 1], positions) * head_size ** (-0.5)
    value = summed[:, 2]
    gate = summed[:, 3]
    heads = (lax.axis_index("tp") * head_dev + jnp.arange(head_dev)).astype(jnp.float32)
    gamma = 1.0 - 2.0 ** (-5.0 - 5.0 * heads / (HEADS - 1))
    new_state = gamma[None, :, None, None] * state + key_rows[:, :, :, None] * value[:, :, None, :]
    read = jnp.einsum("bhd,bhde->bhe", query, new_state, precision=lax.Precision.HIGHEST)
    read = read * lax.rsqrt(jnp.mean(read * read, axis=-1, keepdims=True) + 1e-06)
    retained = (
        (read * jax.nn.silu(gate)).reshape(local_seqs, head_dev * head_size).astype(jnp.bfloat16)
    )
    head_terms = jnp.dot(
        lax.all_gather(retained, "kv", axis=0, tiled=True),
        w_out,
        preferred_element_type=jnp.float32,
    )
    mixed = (inputs + lax.psum(head_terms, "tp")).astype(jnp.bfloat16)
    middle = mixed.astype(jnp.float32)
    squares2 = jnp.sum(middle * middle, axis=1)
    normed2 = (middle * mlp_gain).astype(jnp.bfloat16)
    upward = jnp.dot(normed2, w_up, preferred_element_type=jnp.float32)
    up_full, total_sq2 = lax.psum((upward, squares2), "kv")
    scale2 = lax.rsqrt(total_sq2 / D + 1e-06)
    hidden = jnp.square(jax.nn.relu(up_full * scale2[:, None])).astype(jnp.bfloat16)
    down_terms = jnp.dot(hidden, w_down, preferred_element_type=jnp.float32)
    layer_out = (middle + lax.psum(down_terms, "tp")).astype(jnp.bfloat16)
    return (layer_out, new_state)


def partners(n, i):
    if n == 4:
        return PERMS[i]
    return [tuple(j ^ s for j in range(n)) for s in reversed(range(1, n))]


def inverse(perm):
    return tuple(perm.index(j) for j in range(len(perm)))


def lookup(axis, perm):
    me = lax.axis_index(axis)
    return sum(jnp.where(me == j, entry, 0) for j, entry in enumerate(perm))


def exchange(values, axis, perms):
    if not isinstance(values, list):
        values = [values] * len(perms)
    got = []
    for value, perm in zip(values, perms):
        got.append(lax.ppermute(value, axis, list(enumerate(perm))))
    return got


def pieces(value):
    high = value.astype(BF16).astype(F32)
    rest = value - high
    middle = rest.astype(BF16).astype(F32)
    return high, middle, rest - middle


def reorder(perms, values):
    rows = values.shape[0]
    block = rows // len(perms)
    to = lax.broadcasted_iota(jnp.int32, (rows, rows), 0)
    of = lax.broadcasted_iota(jnp.int32, (rows, rows), 1)
    owner = sum(jnp.where(to // block == k, lookup("kv", perm), 0) for k, perm in enumerate(perms))
    hot = owner * block + to % block == of
    return jnp.dot(hot.astype(F32).astype(BF16), values, preferred_element_type=F32)


def project_kernel(perms, chunks, flight, x_hbm, gain_hbm, *refs):
    n = len(perms)
    weights, outs, (x_ref, gain_ref, held, sems, small) = refs[:4], refs[4 : 4 + n], refs[4 + n :]
    first = [
        pltpu.make_async_copy(x_hbm, x_ref, small.at[0]),
        pltpu.make_async_copy(gain_hbm, gain_ref, small.at[1]),
    ]
    rows, depth = x_ref.shape
    width = held.shape[2]
    block, heads = rows // n, width // LANES
    step = depth // chunks
    copies = []
    for i, w in enumerate(weights):
        for j in range(chunks):
            part = pl.ds(j * step, step)
            copies.append(pltpu.make_async_copy(w.at[part], held.at[i, part], sems.at[i, j]))
    for copy in first + copies[:flight]:
        copy.start()
    first[0].wait()
    x = reorder(perms, x_ref[...])
    lane = lax.broadcasted_iota(jnp.int32, (rows, LANES), 1)
    high, mid, low = pieces(jnp.sum(x * x, axis=1, keepdims=True))
    split = jnp.where(lane == 0, high, jnp.where(lane == 1, mid, jnp.where(lane == 2, low, 0.0)))
    group = heads * block
    for s, out in enumerate(outs):
        mine = split[s * block : (s + 1) * block]
        out[4 * group :] = jnp.concatenate([mine] * heads, axis=0).astype(out.dtype)
    first[1].wait()
    normed = (x * gain_ref[...]).astype(BF16)
    for i in range(4):
        total = None
        for j in range(chunks):
            at = chunks * i + j
            copies[at].wait()
            if at + flight < len(copies):
                copies[at + flight].start()
            part = slice(j * step, (j + 1) * step)
            term = jnp.dot(normed[:, part], held[i, part], preferred_element_type=F32)
            total = term if total is None else total + term
        for s, out in enumerate(outs):
            mine = total[s * block : (s + 1) * block]
            mine = jnp.concatenate([mine[:, h * LANES : (h + 1) * LANES] for h in range(heads)], axis=0)
            out[i * group : (i + 1) * group] = mine.astype(out.dtype)


def prepare_kernel(state_hbm, cos_ref, sin_ref, out_ref, cosine_ref, sine_ref, gamma_ref, state_ref, sem):
    block, head_dev, size, _ = state_ref.shape
    copy = pltpu.make_async_copy(state_hbm, state_ref, sem)
    copy.start()
    copy.wait()
    for h in range(head_dev):
        for b in range(block):
            value = state_ref[b, h]
            high = value.astype(BF16)
            at = slice(b * size, (b + 1) * size)
            out_ref[h, :size, at] = high
            out_ref[h, size:, at] = (value - high.astype(F32)).astype(BF16)
    cos, sin = cos_ref[...], sin_ref[...]
    cosine_ref[...] = jnp.concatenate([jnp.concatenate([cos, cos], axis=1)] * head_dev, axis=0)
    sine_ref[...] = jnp.concatenate([jnp.concatenate([-sin, sin], axis=1)] * head_dev, axis=0)
    row = lax.broadcasted_iota(jnp.int32, gamma_ref.shape, 0)
    head = lax.axis_index("tp") * head_dev + row // block
    gamma_ref[...] = 1.0 - jnp.exp2(-5.0 - 5.0 * head.astype(F32) / (HEADS - 1))


def read_kernel(n, block, own_ref, *refs):
    got, (cos_ref, sin_ref, gamma_ref, prep_ref, kept_ref, key_ref, value_ref) = refs[: n - 1], refs[n - 1 :]
    head_dev, _, wide = prep_ref.shape
    size = wide // block
    total = own_ref[...]
    for g in got:
        total = total + g[...].astype(F32)
    group = head_dev * block
    sq = total[4 * group :]
    scale = lax.rsqrt((sq[:, 0:1] + sq[:, 1:2] + sq[:, 2:3]) / D + 1e-06)
    query, key, value, gate = (total[i * group : (i + 1) * group] * scale for i in range(4))
    cos, sin = cos_ref[...], sin_ref[...]
    query = query * cos + pltpu.roll(query, size // 2, 1) * sin
    high = query.astype(BF16).astype(F32)
    low = query - high
    row = lax.broadcasted_iota(jnp.int32, (2 * block, size), 0)
    reads = []
    for h in range(head_dev):
        at = slice(h * block, (h + 1) * block)
        both = jnp.concatenate([high[at], low[at]], axis=0).astype(BF16)
        both = jnp.concatenate([both, both], axis=1)
        product = jnp.dot(both, prep_ref[h], preferred_element_type=F32)
        picked = jnp.zeros((2 * block, size), F32)
        for b in range(block):
            picked = jnp.where(row % block == b, product[:, b * size : (b + 1) * size], picked)
        reads.append(picked[:block] + picked[block:])
    key = (key * cos + pltpu.roll(key, size // 2, 1) * sin) * size ** (-0.5)
    key_ref[...] = key
    value_ref[...] = value
    match = jnp.sum(query * key, axis=1, keepdims=True)
    gate = gate / (1.0 + jnp.exp(-gate))
    read = gamma_ref[...] * jnp.concatenate(reads, axis=0) + match * value
    read = read * lax.rsqrt(jnp.mean(read * read, axis=1, keepdims=True) + 1e-06)
    kept_ref[...] = (read * gate).astype(BF16)


def update_kernel(key_ref, value_ref, gamma_ref, after_ref, state_ref, new_hbm, new_ref, sems):
    del after_ref
    block, head_dev, _, _ = state_ref.shape
    copies = []
    for h in range(head_dev):
        rows = slice(h * block, (h + 1) * block)
        k, v = key_ref[rows], value_ref[rows]
        columns = jnp.concatenate([k, k], axis=0).T
        gamma = gamma_ref[h * block : h * block + 1, :]
        for b in range(block):
            new_ref[b, h] = gamma * state_ref[b, h] + columns[:, b : b + 1] * v[b : b + 1]
            copies.append(pltpu.make_async_copy(new_ref.at[b, h], new_hbm.at[b, h], sems.at[b, h]))
            copies[-1].start()
    for copy in copies:
        copy.wait()


def out_kernel(perms, *refs):
    n = len(perms)
    parts, (w_ref, own_ref, sent_ref) = refs[:n], refs[n:]
    size = parts[0].shape[1]
    heads = w_ref.shape[0] // size
    block = parts[0].shape[0] // heads
    values = [p[...].astype(F32) for p in parts]
    places = [lookup("kv", inverse(perm)) for perm in perms]
    ordered = []
    for t in range(n):
        value = values[0]
        for place, other in zip(places[1:], values[1:]):
            value = jnp.where(place == t, other, value)
        ordered.append(value)
    columns = [
        jnp.concatenate([value[h * block : (h + 1) * block] for value in ordered], axis=0) for h in range(heads)
    ]
    kept = jnp.concatenate(columns, axis=1).astype(BF16)
    terms = jnp.dot(kept, w_ref[...], preferred_element_type=F32)
    own_ref[...] = terms
    sent_ref[...] = terms.astype(BF16)


def up_kernel(n_tp, perms, x_ref, gain_ref, w_ref, own_ref, *refs):
    got, (mixed_ref, normed_ref, split_ref, *sent) = refs[: n_tp - 1], refs[n_tp - 1 :]
    total = own_ref[...]
    for g in got:
        total = total + g[...].astype(F32)
    mixed = (x_ref[...].astype(F32) + total).astype(BF16)
    mixed_ref[...] = mixed
    middle = mixed.astype(F32)
    normed = (middle * gain_ref[...]).astype(BF16)
    normed_ref[...] = normed
    rows = middle.shape[0]
    high, mid, low = pieces(jnp.sum(middle * middle, axis=1, keepdims=True))
    lane = lax.broadcasted_iota(jnp.int32, (rows, LANES), 1)
    split = jnp.where(lane == 0, high, jnp.where(lane == 1, mid, jnp.where(lane == 2, low, 0.0)))
    split_ref[...] = split
    part = sent[0].shape[1] - LANES
    for perm, out in zip(perms, sent):
        at = pl.ds(pl.multiple_of(lookup("kv", perm) * part, part), part)
        out[:, :part] = jnp.dot(normed, w_ref[:, at], preferred_element_type=F32).astype(out.dtype)
        out[:, part:] = split.astype(out.dtype)


def up_own_kernel(n, normed_ref, w_ref, out_ref):
    part = w_ref.shape[1] // n
    at = pl.ds(pl.multiple_of(lax.axis_index("kv") * part, part), part)
    out_ref[...] = jnp.dot(normed_ref[...], w_ref[:, at], preferred_element_type=F32)


def hidden_kernel(own_ref, split_ref, *refs):
    *got, out_ref = refs
    part = out_ref.shape[1]
    total, split = own_ref[...], split_ref[...]
    for g in got:
        total = total + g[:, :part].astype(F32)
        split = split + g[:, part:].astype(F32)
    sq = split[:, 0:1] + split[:, 1:2] + split[:, 2:3]
    scale = lax.rsqrt(sq / D + 1e-06)
    out_ref[...] = jnp.square(jnp.maximum(total * scale, 0.0)).astype(BF16)


def down_kernel(perm, first, last, *refs):
    part_ref, w_ref, *refs = refs
    part = part_ref.shape[1]
    at = pl.ds(pl.multiple_of(lookup("kv", inverse(perm)) * part, part), part)
    total = jnp.dot(part_ref[...], w_ref[at, :], preferred_element_type=F32)
    if not first:
        total = total + refs.pop(0)[...]
    refs[0][...] = total
    if last:
        refs[1][...] = total.astype(BF16)


def final_kernel(mixed_ref, own_ref, *refs):
    *got, out_ref = refs
    total = own_ref[...]
    for g in got:
        total = total + g[...].astype(F32)
    out_ref[...] = (mixed_ref[...].astype(F32) + total).astype(BF16)


VMEM = pl.BlockSpec(memory_space=pltpu.VMEM)
HBM = pl.BlockSpec(memory_space=pltpu.HBM)


def call(kernel, outs, *args, specs=None, out_specs=None, scratch=(), limit=8, us=1, kept=True):
    return pl.pallas_call(
        kernel,
        out_shape=[(pltpu.VMEM if kept else jax.ShapeDtypeStruct)(*o) for o in outs],
        in_specs=specs or [VMEM] * len(args),
        out_specs=out_specs or [VMEM] * len(outs),
        scratch_shapes=scratch,
        compiler_params=pltpu.CompilerParams(vmem_limit_bytes=limit << 20),
        cost_estimate=pl.CostEstimate(flops=int(us * RATE), bytes_accessed=0, transcendentals=0),
    )(*args)


def far(value):
    return pltpu.with_memory_space_constraint(value, pltpu.HBM)


def near(value):
    return pltpu.with_memory_space_constraint(value, pltpu.VMEM)


def make_direct(n, n_tp):
    def shards(
        tokens, positions, state, norm_gain, w_query, w_key, w_value, w_gate, w_out, mlp_gain, w_up, w_down
    ):
        block, head_dev, size, _ = state.shape
        rows, depth = tokens.shape
        width = head_dev * size
        group = head_dev * block
        chunks, flight = 1, 4
        same = tuple(range(n))
        perms = partners(n, 0)
        own, *sent = call(
            functools.partial(project_kernel, [same, *perms], chunks, flight),
            [((5 * group, size), F32)] + [((5 * group, size), BF16)] * (n - 1),
            far(tokens),
            far(norm_gain[None]),
            far(w_query),
            far(w_key),
            far(w_value),
            far(w_gate),
            specs=[HBM] * 6,
            scratch=[
                pltpu.VMEM((rows, depth), BF16),
                pltpu.VMEM((1, depth), F32),
                pltpu.VMEM((4, depth, width), BF16),
                pltpu.SemaphoreType.DMA((4, chunks)),
                pltpu.SemaphoreType.DMA((2,)),
            ],
            us=2,
        )
        got = exchange(sent, "kv", perms)
        half = size // 2
        freq = 10000.0 ** (-(jnp.arange(half, dtype=F32) * 2.0) / size)
        angle = positions.astype(F32)[:, None] * freq[None, :]
        cosine, sine = jnp.cos(angle), jnp.sin(angle)
        prepared, cosine, sine, gamma = call(
            prepare_kernel,
            [((head_dev, 2 * size, block * size), BF16)] + [((group, size), F32)] * 3,
            far(state),
            cosine,
            sine,
            specs=[HBM, VMEM, VMEM],
            scratch=[pltpu.VMEM(state.shape, F32), pltpu.SemaphoreType.DMA],
        )
        kept, key, value = call(
            functools.partial(read_kernel, n, block),
            [((group, size), BF16), ((group, size), F32), ((group, size), F32)],
            own,
            *got,
            cosine,
            sine,
            gamma,
            prepared,
        )
        perms = partners(n, 1)
        got = exchange(kept, "kv", perms)
        own, sent = call(
            functools.partial(out_kernel, [same, *perms]),
            [((rows, depth), F32), ((rows, depth), BF16)],
            kept,
            *got,
            near(w_out),
        )
        got = exchange(sent, "tp", partners(n_tp, 2))
        part = w_up.shape[1] // n
        w_up = near(w_up)
        perms = partners(n, 3)
        mixed, normed, split, *sent = call(
            functools.partial(up_kernel, n_tp, perms),
            [((rows, depth), BF16), ((rows, depth), BF16), ((rows, LANES), F32)]
            + [((rows, part + LANES), BF16)] * (n - 1),
            tokens,
            mlp_gain[None],
            w_up,
            own,
            *got,
        )
        got = exchange(sent, "kv", perms)
        (new_state,) = call(
            update_kernel,
            [(state.shape, F32)],
            key,
            value,
            gamma,
            split,
            near(state),
            out_specs=[HBM],
            scratch=[pltpu.VMEM(state.shape, F32), pltpu.SemaphoreType.DMA((block, head_dev))],
            kept=False,
        )
        (own,) = call(functools.partial(up_own_kernel, n), [((rows, part), F32)], normed, w_up)
        (hidden,) = call(hidden_kernel, [((rows, part), BF16)], own, split, *got)
        perms = partners(n, 4)
        got = exchange(hidden, "kv", perms)
        w_down = near(w_down)
        (own,) = call(functools.partial(down_kernel, same, True, False), [((rows, depth), F32)], hidden, w_down)
        turns = TURNS if n == 4 else range(n - 1)
        for k in turns:
            last = k == turns[-1]
            own, *sent = call(
                functools.partial(down_kernel, perms[k], False, last),
                [((rows, depth), F32)] + [((rows, depth), BF16)] * last,
                got[k],
                w_down,
                own,
            )
        (sent,) = sent
        got = exchange(sent, "tp", partners(n_tp, 5))
        (layer_out,) = call(final_kernel, [((rows, depth), BF16)], mixed, own, *got, kept=False)
        return (layer_out, new_state)

    return shards


def solution(mesh):
    n_kv, n_tp = mesh.shape["kv"], mesh.shape["tp"]
    direct = all(n <= DIRECT and n & (n - 1) == 0 for n in (n_kv, n_tp))
    return jax.shard_map(
        make_direct(n_kv, n_tp) if direct else shards_large,
        mesh=mesh,
        in_specs=(
            P("grp", "kv"),
            P(("grp", "kv")),
            P(("grp", "kv"), "tp", None, None),
            P("kv"),
            P("kv", "tp"),
            P("kv", "tp"),
            P("kv", "tp"),
            P("kv", "tp"),
            P("tp", "kv"),
            P("kv"),
            P("kv", "tp"),
            P("tp", "kv"),
        ),
        out_specs=(P("grp", "kv"), P(("grp", "kv"), "tp", None, None)),
        check_vma=False,
    )
```
